512 devices in a mesh: sp: 32 (over z, x), tp: 16 (over y, core).
Axes of the slice: x: 4, y: 8, z: 8, core: 2. Of those that a mesh axis runs over, the one named last changes fastest.
Arguments:
- residual: bfloat16 [8192, 2048], P('sp', 'tp'), may hold values from -26 to 26
- queries: bfloat16 [2048, 8192], P('tp', 'sp'), may hold values from -6 to 6
- keys: bfloat16 [2048, 8192], P('tp', 'sp'), may hold values from -6 to 6
- values: bfloat16 [2048, 8192], P('tp', 'sp'), may hold values from -12 to 12
- forget_cache: float32 [32, 8192], P('tp', 'sp'), as said below
- out_weight: bfloat16 [2048, 2048], P('tp'), may hold values from -0.125 to 0.125
- norm_gain: float32 [2048], replicated, may hold values from 0.1 to 1.9
- routes: int32 [8192, 2], P('sp'), may hold values from 0 to 31, all different within a row; in each aligned block of 256 rows (0 to 255, 256 to 511, ...) at most 20 rows name the same one
- route_weight: float32 [8192, 2], P('sp'), may hold values from 0.2 to 1
- gate_weight: bfloat16 [32, 2048, 4096], P('sp', None, 'tp'), may hold values from -0.125 to 0.125
- up_weight: bfloat16 [32, 2048, 4096], P('sp', None, 'tp'), may hold values from -0.125 to 0.125
- down_weight: bfloat16 [32, 4096, 2048], P('sp', 'tp'), may hold values from -0.09375 to 0.09375
Outputs:
- updated: bfloat16 [8192, 2048], P('sp', 'tp')
The draws below stay inside these ranges and needn't reach their ends.
Inputs may be any that keep to these rules, and one draw needn't show every extreme that they name: `routes`: each row names 2 different experts; within the 256 rows of one index of sp no expert is named by more than 20 rows, and in the rows of some index some expert is named by exactly 20. `forget_cache`: each head's row never rises from one position to the next.
All inputs are finite; a program needn't handle non-finite values.
Results may differ from the reference program's by a relative error of at most 0.013.
Values may be sent and summed in bfloat16 or wider, within the bound.
No kernel may reach another device: no remote copies, remote signals or barrier semaphores. Data moves between devices by JAX's collectives and lax.ppermute only.
A program may use at most 64 MiB of HBM per device.

```python
import math
import jax
import jax.numpy as jnp
import numpy as np
from jax import lax

D = 2048
HEAD_TOTAL = 32
HEAD_DIM = 64
FF = 4096
TOPK = 2
TOK_DEV = 256
TOKEN_TOTAL = 8192
EXPERTS = 32
CAP = 20
GROUP_HEADS = 2
FF_PART = 256
N_SP = 32
N_TP = 16


def draw_queries(key, part):
    full_shape = (HEAD_TOTAL * HEAD_DIM, TOKEN_TOTAL)
    drawn = jnp.clip(1.6 * jax.random.normal(jax.random.fold_in(key, 1), full_shape, jnp.float32), -6.0, 6.0)
    return drawn.astype(jnp.bfloat16)


def draw_keys(key, part):
    full_shape = (HEAD_TOTAL * HEAD_DIM, TOKEN_TOTAL)
    drawn = jnp.clip(1.6 * jax.random.normal(jax.random.fold_in(key, 2), full_shape, jnp.float32), -6.0, 6.0)
    return drawn.astype(jnp.bfloat16)


def draw_residual(key, part):
    sequence_lanes = jax.random.split(jax.random.fold_in(key, 3), 3)
    feature = jnp.arange(D, dtype=jnp.float32) / D - 0.5
    jitter = jnp.exp(jax.random.uniform(sequence_lanes[1], (D,), jnp.float32, jnp.log(0.7), jnp.log(1.4)))
    rising = jnp.exp(jnp.log(4.0) * feature) * jitter
    token_scale = jnp.exp(jax.random.uniform(sequence_lanes[2], (TOKEN_TOTAL, 1), jnp.float32, jnp.log(0.3), jnp.log(3.0)))
    drawn = jnp.clip(jax.random.normal(sequence_lanes[0], (TOKEN_TOTAL, D), jnp.float32), -3.0, 3.0)
    return (drawn * rising[None, :] * token_scale).astype(jnp.bfloat16)


def draw_forget_cache(key, part):
    sequence_lanes = jax.random.split(jax.random.fold_in(key, 4), 7)
    head_order = jax.random.permutation(sequence_lanes[0], HEAD_TOTAL)
    slow_count = HEAD_TOTAL // 2
    slow_total = jax.random.uniform(sequence_lanes[1], (HEAD_TOTAL,), jnp.float32, 0.3, 0.9)
    lagging_heads = head_order < slow_count
    fast_length = jax.random.uniform(sequence_lanes[2], (HEAD_TOTAL,), jnp.float32, 30.0, 100.0)
    base_rate = jnp.where(lagging_heads, slow_total / TOKEN_TOTAL, 1.0 / fast_length)
    block_factor = jnp.exp(jax.random.uniform(sequence_lanes[3], (HEAD_TOTAL, TOKEN_TOTAL // TOK_DEV), jnp.float32, jnp.log(0.5), jnp.log(2.0)))
    roughness = jnp.exp(jax.random.uniform(sequence_lanes[4], (HEAD_TOTAL, TOKEN_TOTAL), jnp.float32, jnp.log(0.5), jnp.log(2.0)))
    decay_speed = base_rate[:, None] * jnp.repeat(block_factor, TOK_DEV, axis=1) * roughness
    spike_locations = jax.random.randint(sequence_lanes[5], (2,), 0, TOKEN_TOTAL)
    spike_struck = jnp.any(jnp.arange(TOKEN_TOTAL, dtype=jnp.int32)[:, None] == spike_locations[None, :], axis=1)
    spike_retained = jnp.log(jax.random.uniform(sequence_lanes[6], (HEAD_TOTAL,), jnp.float32, 0.55, 0.8))
    gate_logarithm = -decay_speed + jnp.where(lagging_heads[:, None] & spike_struck[None, :], spike_retained[:, None], 0.0)
    return jnp.cumsum(gate_logarithm, axis=1).astype(jnp.float32)


def block_scale(rng, shape, cuts, low, high):
    def one(dim, shards_of):
        draws = jax.random.uniform(jax.random.fold_in(jax.random.fold_in(rng, 6), dim), (shards_of,), jnp.float32, low / len(cuts), high / len(cuts))
        return jnp.repeat(jnp.exp(draws), shape[dim] // shards_of).reshape((-1,) + (1,) * (len(shape) - dim - 1))

    level = one(*cuts[0])
    for cut in cuts[1:]:
        level = level * one(*cut)
    return level


def routed_block(stream_key, own, number, rows, count, top, limit, skew):
    order = jax.random.permutation(stream_key, count)
    packed, ordinary = shares(count, rows * top, limit, skew, True), shares(count, rows * top, limit, skew, False)
    places = jnp.arange(count)

    def named(sizes, rotation):
        used = int((sizes > 0).sum())
        fixed = max(1, used // 4)
        shifted = fixed + (places - fixed + rotation * (used - fixed)) % max(1, count - fixed)
        return jnp.zeros((count,), jnp.int32).at[order[jnp.where(places < fixed, places, shifted)]].set(jnp.asarray(sizes, jnp.int32))

    sizes = jnp.where(number % 4 == 0, named(packed, number // 4), named(ordinary, number - number // 4 - 1))
    mixed = jax.random.permutation(jax.random.fold_in(own, 3), count)
    giver, taker = mixed[0:count // 2 * 2:2], mixed[1:count // 2 * 2:2]
    room = jnp.minimum(sizes[giver] - 1, limit - sizes[taker]) // 2
    room = jnp.where((giver == order[0]) | (taker == order[0]) | (sizes[taker] == 0), 0, jnp.maximum(room, 0))
    shifted = jax.random.randint(jax.random.fold_in(own, 4), (count // 2,), 0, 1 << 20) % (room + 1)
    sizes = sizes.at[giver].add(-shifted).at[taker].add(shifted)
    labels = jnp.searchsorted(jnp.cumsum(sizes), jnp.arange(rows * top), side="right").astype(jnp.int32)
    listing = labels.reshape(top, rows).T
    listing = listing[jax.random.permutation(jax.random.fold_in(own, 1), rows)]
    rotation = jax.random.randint(jax.random.fold_in(own, 2), (rows, 1), 0, top)
    return jnp.take_along_axis(listing, (jnp.arange(top)[None, :] + rotation) % top, axis=1)


def shares(amount, total, reach, skew, full):
    weights = [(1 << 20) // math.isqrt(rank ** skew) + 1 for rank in range(1, amount + 1)]
    largest = reach if full else min(reach, max(-(-total // amount), total * weights[0] // sum(weights)))
    least = 1 if total - largest >= amount - 1 else 0
    counts, spare = [largest] + [least] * (amount - 1), total - largest - least * (amount - 1)
    while spare > 0:
        candidates = [i for i in range(1, amount) if counts[i] < largest] or [i for i in range(1, amount) if counts[i] < reach]
        whole, left = sum([weights[i] for i in candidates]), spare
        for i in candidates:
            more = min(reach - counts[i], max(1, left * weights[i] // whole), spare)
            counts[i] = counts[i] + more
            spare = spare - more
    return np.array(counts)


def bell_draw(stream_key, shape, scale, bound, pieces=(), kind=jnp.bfloat16):
    array = jax.random.normal(stream_key, shape, jnp.float32) * scale
    if len(pieces) > 0:
        array = block_scale(stream_key, shape, pieces, -0.22, 0.18) * array
    return jnp.clip(array, min=-bound, max=bound).astype(kind)


def setup_inputs(seed: int = 0) -> dict:
    seeds = jax.random.split(jax.random.key(seed), 13)
    residual = draw_residual(jax.random.fold_in(seeds[12], 71), 0)
    queries = draw_queries(jax.random.fold_in(seeds[12], 71), 0)
    keys = draw_keys(jax.random.fold_in(seeds[12], 71), 0)
    values = bell_draw(seeds[3], (HEAD_TOTAL * HEAD_DIM, TOKEN_TOTAL), 2.0, 12.0, ((0, 16), (1, 32)))
    forget_cache = draw_forget_cache(jax.random.fold_in(seeds[12], 71), 0)
    out_weight = bell_draw(seeds[5], (HEAD_TOTAL * HEAD_DIM, D), (HEAD_TOTAL * HEAD_DIM) ** -0.5, 0.125, ((0, 16),))
    norm_gain = jnp.clip(1.0 + 0.18 * jax.random.normal(seeds[6], (D,), jnp.float32), 0.1, 1.9)
    routes_keys = jax.random.split(jax.random.fold_in(seeds[7], 1), TOKEN_TOTAL // TOK_DEV)
    routes_turns = jax.random.permutation(jax.random.fold_in(seeds[7], 3), TOKEN_TOTAL // TOK_DEV)
    routes = jax.vmap(lambda own, number: routed_block(jax.random.fold_in(seeds[7], 2), own, number, TOK_DEV, EXPERTS, TOPK, CAP, 0))(routes_keys, routes_turns).reshape((TOKEN_TOTAL, TOPK))
    route_weight = jnp.clip(0.2 + 0.8 * jax.random.uniform(seeds[8], (TOKEN_TOTAL, TOPK), jnp.float32) ** block_scale(seeds[8], (TOKEN_TOTAL, TOPK), ((0, 32),), -0.2, 0.2), 0.2, 1.0)
    gate_weight = bell_draw(seeds[9], (EXPERTS, D, FF), D ** -0.5, 0.125, ((0, 32), (2, 16)))
    up_weight = bell_draw(seeds[10], (EXPERTS, D, FF), D ** -0.5, 0.125, ((0, 32), (2, 16)))
    down_weight = bell_draw(seeds[11], (EXPERTS, FF, D), FF ** -0.5, 0.09375, ((0, 32), (1, 16)))
    return {"residual": residual, "queries": queries, "keys": keys, "values": values, "forget_cache": forget_cache, "out_weight": out_weight, "norm_gain": norm_gain, "routes": routes, "route_weight": route_weight, "gate_weight": gate_weight, "up_weight": up_weight, "down_weight": down_weight}


norm_eps = 1e-06

def attend_head(operands):
    query_rows, key_rows, value_rows, cumulative = operands
    block_span = TOKEN_TOTAL // 8
    position = jnp.arange(TOKEN_TOTAL, dtype=jnp.int32)
    blocks = []
    for block_index in range(8):
        first_row = block_index * block_span
        end_row = first_row + block_span
        scores = jnp.dot(query_rows[:, first_row:end_row].T, key_rows[:, :end_row], preferred_element_type=jnp.float32) * HEAD_DIM ** (-0.5)
        scores = scores + cumulative[first_row:end_row, None] - cumulative[None, :end_row]
        allowed = position[None, :end_row] <= position[first_row:end_row, None]
        scores = jnp.where(allowed, scores, -jnp.inf)
        weights = jnp.exp(scores - lax.optimization_barrier(jnp.max(scores, axis=1, keepdims=True)))
        totals = lax.optimization_barrier(jnp.sum(weights, axis=1, keepdims=True))
        blocks.append(jnp.dot(weights.astype(jnp.bfloat16), value_rows[:, :end_row].T, preferred_element_type=jnp.float32) / totals)
    return jnp.concatenate(blocks, axis=0).astype(jnp.bfloat16)

def reference(residual, queries, keys, values, forget_cache, out_weight, norm_gain, routes, route_weight, gate_weight, up_weight, down_weight):
    query_heads = queries.reshape(HEAD_TOTAL, HEAD_DIM, TOKEN_TOTAL)
    key_heads = keys.reshape(HEAD_TOTAL, HEAD_DIM, TOKEN_TOTAL)
    value_heads = values.reshape(HEAD_TOTAL, HEAD_DIM, TOKEN_TOTAL)
    attended = lax.map(attend_head, (query_heads, key_heads, value_heads, forget_cache))
    attended = attended.transpose(1, 0, 2).reshape(TOKEN_TOTAL, HEAD_TOTAL * HEAD_DIM)
    group_width = GROUP_HEADS * HEAD_DIM

    def add_group(running, group_index):
        offset = (group_index * group_width).astype(jnp.int32)
        group_rows = lax.dynamic_slice_in_dim(attended, offset, group_width, 1)
        weight_rows = lax.dynamic_slice_in_dim(out_weight, offset, group_width, 0)
        group_part = lax.optimization_barrier(jnp.dot(group_rows, weight_rows, preferred_element_type=jnp.float32).astype(jnp.bfloat16))
        return (running + group_part.astype(jnp.float32), None)
    head_sum, _ = lax.scan(add_group, jnp.zeros((TOKEN_TOTAL, D), jnp.float32), jnp.arange(N_TP, dtype=jnp.int32))
    stream = (residual.astype(jnp.float32) + head_sum).astype(jnp.bfloat16)
    widened = stream.astype(jnp.float32)
    normed = (widened * lax.rsqrt(lax.optimization_barrier(jnp.mean(widened * widened, axis=1, keepdims=True)) + norm_eps) * norm_gain.astype(jnp.float32)).astype(jnp.bfloat16)
    most_rows = N_SP * CAP

    def add_expert(running, expert):
        chosen = routes == expert
        picked_any = jnp.any(chosen, axis=1)
        row_order = jnp.argsort(jnp.where(picked_any, 0, 1).astype(jnp.int32), stable=True)[:most_rows].astype(jnp.int32)
        slot_rows = jnp.take(normed, row_order, axis=0)
        row_share = lax.optimization_barrier(jnp.sum(jnp.where(chosen, route_weight, jnp.zeros_like(route_weight)), axis=1))[row_order]
        gate_value = jnp.dot(slot_rows, gate_weight[expert], preferred_element_type=jnp.float32)
        up_value = jnp.dot(slot_rows, up_weight[expert], preferred_element_type=jnp.float32)
        hidden = (jax.nn.silu(gate_value) * up_value).astype(jnp.bfloat16)
        expert_parts = jnp.einsum('rpf,pfd->prd', hidden.reshape(most_rows, N_TP, FF_PART).astype(jnp.float32), down_weight[expert].reshape(N_TP, FF_PART, D).astype(jnp.float32))
        expert_parts = lax.optimization_barrier(expert_parts.astype(jnp.bfloat16))
        expert_out = lax.optimization_barrier(jnp.sum(expert_parts.astype(jnp.float32), axis=0)).astype(jnp.bfloat16)
        return (running.at[row_order].add(row_share[:, None] * expert_out.astype(jnp.float32)), None)
    mixture, _ = lax.scan(add_expert, jnp.zeros((TOKEN_TOTAL, D), jnp.float32), jnp.arange(EXPERTS, dtype=jnp.int32))
    return (stream.astype(jnp.float32) + mixture).astype(jnp.bfloat16)
```

```python
import functools

import jax
import jax.numpy as jnp
from jax import lax
from jax.experimental import pallas as pl
from jax.experimental.pallas import tpu as pltpu
from jax.sharding import Mesh
from jax.sharding import PartitionSpec as P

SP = ("z", "x")
TP = ("y", "c")
INTERPRET = False

norm_eps = 1e-06
masked_score = -1e30
extra_rows = 16
lane = 128


def split_three(full):
    first = lax.reduce_precision(full, 8, 7)
    second = lax.reduce_precision(full - first, 8, 7)
    third = lax.reduce_precision(full - first - second, 8, 7)
    return [part.astype(jnp.bfloat16) for part in (first, second, third)]


def sent_to_all(shard, axis):
    copies = jnp.broadcast_to(shard, (lax.axis_size(axis), *shard.shape))
    return lax.all_to_all(copies, axis, split_axis=0, concat_axis=0, tiled=True)


def swapped(shard):
    return lax.ppermute(shard, "c", [(0, 1), (1, 0)])


def attend_kernel(head_count, head_width, place_ref, kv_ref, *refs):
    x_count = len(refs) - 4
    query_refs = refs[:x_count]
    out_ref, query_scratch, sum_scratch, peak_scratch = refs[x_count:]
    tokens = kv_ref.shape[2]
    deep = head_width + extra_rows
    z_place, x_place = place_ref[0], place_ref[1]
    row = lax.broadcasted_iota(jnp.int32, (extra_rows, tokens), 0)
    minus = jnp.where(row < 3, -1.0, 0.0).astype(jnp.bfloat16)
    ones = jnp.ones((extra_rows, tokens), jnp.bfloat16)
    for head in range(head_count):
        for shift in range(x_count):
            chain = head * x_count + shift
            query_scratch[chain, :head_width] = query_refs[shift][
                head * head_width : (head + 1) * head_width
            ]
            query_scratch[chain, head_width:] = minus
            sum_scratch[chain] = jnp.zeros((deep, tokens), jnp.float32)
            peak_scratch[chain] = jnp.full((8, tokens), masked_score, jnp.float32)

    def one(chain, key_rows, value_rows, masked):
        scores = lax.dot_general(
            key_rows,
            query_scratch[chain],
            (((0,), (0,)), ((), ())),
            preferred_element_type=jnp.float32,
        )
        if masked:
            key_place = lax.broadcasted_iota(jnp.int32, scores.shape, 0)
            query_place = lax.broadcasted_iota(jnp.int32, scores.shape, 1)
            scores = jnp.where(key_place <= query_place, scores, masked_score)
        old_peak = peak_scratch[chain, :1]
        new_peak = jnp.maximum(old_peak, jnp.max(scores, axis=0, keepdims=True))
        weights = jnp.exp(scores - new_peak).astype(jnp.bfloat16)
        shrink = jnp.exp(old_peak - new_peak)
        sum_scratch[chain] = sum_scratch[chain] * shrink + jnp.dot(
            value_rows, weights, preferred_element_type=jnp.float32
        )
        peak_scratch[chain] = jnp.broadcast_to(new_peak, (8, tokens))

    def loaded(z_key, head):
        key_rows = kv_ref[z_key, head * deep : (head + 1) * deep]
        value_first = head_count * deep + head * head_width
        value_rows = kv_ref[z_key, value_first : value_first + head_width]
        return key_rows, jnp.concatenate([value_rows, ones], axis=0)

    def earlier(z_key, carry):
        for head in range(head_count):
            key_rows, value_rows = loaded(z_key, head)
            for shift in range(x_count):
                one(head * x_count + shift, key_rows, value_rows, False)
        return carry

    lax.fori_loop(0, z_place, earlier, 0)
    for head in range(head_count):
        key_rows, value_rows = loaded(z_place, head)
        one(head * x_count, key_rows, value_rows, True)
    for shift in range(1, x_count):

        @pl.when(x_place < shift)
        def _():
            for head in range(head_count):
                key_rows, value_rows = loaded(z_place, head)
                one(head * x_count + shift, key_rows, value_rows, False)

    for shift in range(x_count):
        target = lax.rem(x_place + x_count - shift, x_count)
        stats = jnp.zeros((extra_rows, tokens), jnp.float32)
        for head in range(head_count):
            chain = head * x_count + shift
            out_ref[target, head * head_width : (head + 1) * head_width] = sum_scratch[
                chain, :head_width
            ].astype(jnp.bfloat16)
            place = head * 6
            for full in (peak_scratch[chain, :1], sum_scratch[chain, head_width : head_width + 1]):
                for _ in range(3):
                    part = full.astype(jnp.bfloat16).astype(jnp.float32)
                    full = full - part
                    stats = jnp.where(row == place, part, stats)
                    place += 1
        out_ref[target, head_count * head_width :] = stats.astype(jnp.bfloat16)


def project_kernel(head_count, head_width, place_ref, parts_ref, weight_ref, mine_ref, other_ref, full_ref):
    x_count = parts_ref.shape[0]
    tp_half = mine_ref.shape[0]
    width = head_count * head_width
    core = place_ref[2]
    rows = []
    for head in range(head_count):
        peaks, totals = [], []
        for part in range(x_count):
            stats = parts_ref[part, width : width + extra_rows].astype(jnp.float32)
            base = head * 6
            peaks.append(stats[base : base + 1] + stats[base + 1 : base + 2] + stats[base + 2 : base + 3])
            totals.append(
                stats[base + 3 : base + 4] + stats[base + 4 : base + 5] + stats[base + 5 : base + 6]
            )
        top = functools.reduce(jnp.maximum, peaks)
        factors = [jnp.exp(peak - top) for peak in peaks]
        total = sum(factor * amount for factor, amount in zip(factors, totals))
        summed = sum(
            parts_ref[part, head * head_width : (head + 1) * head_width].astype(jnp.float32)
            * factors[part]
            for part in range(x_count)
        )
        rows.append((summed / total).astype(jnp.bfloat16))
    attended = jnp.concatenate(rows, axis=0)
    full_ref[...] = lax.dot_general(
        attended, weight_ref[...], (((0,), (0,)), ((), ())), preferred_element_type=jnp.float32
    ).astype(jnp.bfloat16)
    for block in range(tp_half):
        own = pl.multiple_of((block * 2 + core) * lane, lane)
        far = pl.multiple_of((block * 2 + 1 - core) * lane, lane)
        mine_ref[block] = full_ref[:, pl.ds(own, lane)]
        other_ref[block] = full_ref[:, pl.ds(far, lane)]


def expert_kernel(place_ref, own_ref, far_ref, gain_ref, gate_ref, up_ref, down_ref, mine_ref, other_ref, rows_ref, full_ref):
    core = place_ref[2]
    blocks = own_ref.shape[0]
    width = rows_ref.shape[1]
    squares = jnp.zeros(own_ref.shape[1:], jnp.float32)
    for block in range(blocks):
        for source in (own_ref, far_ref):
            values = source[block].astype(jnp.float32)
            squares = squares + values * values
    scale = lax.rsqrt(jnp.sum(squares, axis=1, keepdims=True) / width + norm_eps)
    for block in range(blocks):
        for source, side in ((own_ref, core), (far_ref, 1 - core)):
            index = block * 2 + side
            values = source[block].astype(jnp.float32) * scale * gain_ref[index]
            rows_ref[:, pl.ds(pl.multiple_of(index * lane, lane), lane)] = values.astype(jnp.bfloat16)
    gate = jnp.dot(rows_ref[...], gate_ref[...], preferred_element_type=jnp.float32)
    up = jnp.dot(rows_ref[...], up_ref[...], preferred_element_type=jnp.float32)
    hidden = (gate / (1.0 + jnp.exp(-gate)) * up).astype(jnp.bfloat16)
    full_ref[...] = jnp.dot(hidden, down_ref[...], preferred_element_type=jnp.float32).astype(
        jnp.bfloat16
    )
    for block in range(blocks):
        own = pl.multiple_of((block * 2 + core) * lane, lane)
        far = pl.multiple_of((block * 2 + 1 - core) * lane, lane)
        mine_ref[block] = full_ref[:, pl.ds(own, lane)]
        other_ref[block] = full_ref[:, pl.ds(far, lane)]


def shards(
    residual,
    queries,
    keys,
    values,
    forget_cache,
    out_weight,
    norm_gain,
    routes,
    route_weight,
    gate_weight,
    up_weight,
    down_weight,
):
    z_count, x_count, y_count = (lax.axis_size(axis) for axis in ("z", "x", "y"))
    sp_count = z_count * x_count
    token_count, local_width = residual.shape
    model_width = norm_gain.shape[0]
    head_count = forget_cache.shape[0]
    head_width = queries.shape[0] // head_count
    top_count = routes.shape[1]
    capacity = max(2, token_count * top_count * 5 // (4 * sp_count))
    slot_total = sp_count * capacity
    bf16, f32 = jnp.bfloat16, jnp.float32
    place = jnp.stack(
        [lax.axis_index("z"), lax.axis_index("x"), lax.axis_index("c"), lax.axis_index("y")]
    ).astype(jnp.int32)
    smem = pl.BlockSpec(memory_space=pltpu.SMEM)
    vmem = pl.BlockSpec(memory_space=pltpu.VMEM)

    gates = jnp.stack(split_three(forget_cache), axis=1)
    gates = jnp.pad(gates, ((0, 0), (0, extra_rows - 3), (0, 0)))
    key_rows = jnp.concatenate([keys.reshape(head_count, head_width, token_count), gates], axis=1)
    message = jnp.concatenate([key_rows.reshape(-1, token_count), values], axis=0)
    gathered = sent_to_all(message, "z")
    scaled = queries * jnp.asarray(head_width ** (-0.5), bf16)
    query_list = [scaled] + [
        lax.ppermute(scaled, "x", [(i, (i + shift) % x_count) for i in range(x_count)])
        for shift in range(1, x_count)
    ]
    chains = head_count * x_count
    deep = head_width + extra_rows
    part_rows = head_count * head_width + extra_rows
    parts = pl.pallas_call(
        functools.partial(attend_kernel, head_count, head_width),
        out_shape=jax.ShapeDtypeStruct((x_count, part_rows, token_count), bf16),
        in_specs=[smem] + [vmem] * (1 + x_count),
        out_specs=vmem,
        scratch_shapes=[
            pltpu.VMEM((chains, deep, token_count), bf16),
            pltpu.VMEM((chains, deep, token_count), f32),
            pltpu.VMEM((chains, 8, token_count), f32),
        ],
        name="attend",
        interpret=INTERPRET,
    )(place, gathered, *query_list)

    expert_ids = jnp.arange(sp_count, dtype=jnp.int32)
    chosen = routes[:, :, None] == expert_ids
    named = jnp.any(chosen, axis=1)
    token_ids = jnp.arange(token_count, dtype=jnp.int32)
    before = (token_ids[None, :] < token_ids[:, None]).astype(bf16)
    rank = jnp.dot(before, named.astype(bf16), preferred_element_type=f32).astype(jnp.int32)
    slot_ids = jnp.arange(capacity, dtype=jnp.int32)
    taken = (named.T[:, None, :] & (rank.T[:, None, :] == slot_ids[:, None])).astype(bf16)
    taken = taken.reshape(slot_total, token_count)
    share = jnp.sum(jnp.where(chosen, route_weight[:, :, None], 0.0), axis=1)
    share_first = lax.reduce_precision(share, 8, 7)
    share_rest = (share - share_first).astype(bf16)

    def spread(weights):
        return jnp.where(
            rank[:, :, None] == slot_ids, weights.astype(bf16)[:, :, None], jnp.zeros((), bf16)
        ).reshape(token_count, slot_total)

    give_first, give_rest = spread(share_first), spread(share_rest)

    received = lax.all_to_all(parts, "x", split_axis=0, concat_axis=0, tiled=True)
    half = jax.ShapeDtypeStruct((y_count, token_count, local_width), bf16)
    mine, other = pl.pallas_call(
        functools.partial(project_kernel, head_count, head_width),
        out_shape=(half, half),
        in_specs=[smem, vmem, vmem],
        out_specs=(vmem, vmem),
        scratch_shapes=[pltpu.VMEM((token_count, model_width), bf16)],
        name="project",
        interpret=INTERPRET,
    )(place, received, out_weight)
    paired = (mine.astype(f32) + swapped(other).astype(f32)).astype(bf16)
    pieces = lax.all_to_all(paired, "y", split_axis=0, concat_axis=0, tiled=True)
    head_sum = jnp.sum(pieces.astype(f32), axis=0)
    stream = (residual.astype(f32) + head_sum).astype(bf16)

    sent = jnp.dot(taken, stream, preferred_element_type=f32).astype(bf16)
    arrived = lax.all_to_all(
        sent.reshape(sp_count, capacity, local_width), SP, split_axis=0, concat_axis=0, tiled=True
    ).reshape(slot_total, local_width)
    own = sent_to_all(arrived, "y")
    far = swapped(own)
    row_steps = 2 if slot_total % 32 == 0 else 1
    row_block = slot_total // row_steps
    hidden_units = gate_weight.shape[2]
    row_spec = pl.BlockSpec((y_count, row_block, local_width), lambda i: (0, i, 0))
    half = jax.ShapeDtypeStruct((y_count, slot_total, local_width), bf16)
    mine, other = pl.pallas_call(
        expert_kernel,
        grid=(row_steps,),
        out_shape=(half, half),
        in_specs=[
            smem,
            row_spec,
            row_spec,
            pl.BlockSpec((2 * y_count, 1, lane), lambda i: (0, 0, 0)),
            pl.BlockSpec((model_width, hidden_units), lambda i: (0, 0)),
            pl.BlockSpec((model_width, hidden_units), lambda i: (0, 0)),
            pl.BlockSpec((hidden_units, model_width), lambda i: (0, 0)),
        ],
        out_specs=(row_spec, row_spec),
        scratch_shapes=[
            pltpu.VMEM((row_block, model_width), bf16),
            pltpu.VMEM((row_block, model_width), bf16),
        ],
        name="expert",
        interpret=INTERPRET,
    )(
        place,
        own,
        far,
        norm_gain.reshape(2 * y_count, 1, lane),
        gate_weight[0],
        up_weight[0],
        down_weight[0],
    )
    paired = (mine.astype(f32) + swapped(other).astype(f32)).astype(bf16)
    pieces = lax.all_to_all(paired, "y", split_axis=0, concat_axis=0, tiled=True)
    expert_out = jnp.sum(pieces.astype(f32), axis=0).astype(bf16)
    back = lax.all_to_all(
        expert_out.reshape(sp_count, capacity, local_width), SP, split_axis=0, concat_axis=0, tiled=True
    ).reshape(slot_total, local_width)
    mixture = jnp.dot(give_first, back, preferred_element_type=f32) + jnp.dot(
        give_rest, back, preferred_element_type=f32
    )
    return (stream.astype(f32) + mixture).astype(bf16)


def solution(mesh):
    sp_count, tp_count = mesh.shape["sp"], mesh.shape["tp"]
    x_count = 4 if sp_count % 8 == 0 else 2
    finer = Mesh(
        mesh.devices.reshape(sp_count // x_count, x_count, tp_count // 2, 2), ("z", "x", "y", "c")
    )
    in_specs = (
        P(SP, TP),
        P(TP, SP),
        P(TP, SP),
        P(TP, SP),
        P(TP, SP),
        P(TP, None),
        P(),
        P(SP, None),
        P(SP, None),
        P(SP, None, TP),
        P(SP, None, TP),
        P(SP, TP, None),
    )
    return jax.shard_map(
        shards, mesh=finer, in_specs=in_specs, out_specs=P(SP, TP), check_vma=False
    )
```

```python
import functools

import jax
import jax.numpy as jnp
from jax import lax
from jax.experimental import pallas as pl
from jax.experimental.pallas import tpu as pltpu
from jax.sharding import Mesh
from jax.sharding import PartitionSpec as P


SP = ("z", "x")
TP = ("y", "c")
INTERPRET = False

norm_eps = 1e-06
masked_score = -1e30
extra_rows = 16
lane = 128


def split_three(full):
    first = lax.reduce_precision(full, 8, 7)
    second = lax.reduce_precision(full - first, 8, 7)
    third = lax.reduce_precision(full - first - second, 8, 7)
    return [part.astype(jnp.bfloat16) for part in (first, second, third)]


def sent_to_all(shard, axis):
    copies = jnp.broadcast_to(shard, (lax.axis_size(axis), *shard.shape))
    return lax.all_to_all(copies, axis, split_axis=0, concat_axis=0, tiled=True)


def swapped(shard):
    return lax.ppermute(shard, "c", [(0, 1), (1, 0)])


def attend_kernel(head_count, head_width, place_ref, kv_ref, *refs):
    x_count = len(refs) - 4
    query_refs = refs[:x_count]
    out_ref, query_scratch, sum_scratch, peak_scratch = refs[x_count:]
    tokens = kv_ref.shape[2]
    deep = head_width + extra_rows
    z_place, x_place = place_ref[0], place_ref[1]
    row = lax.broadcasted_iota(jnp.int32, (extra_rows, tokens), 0)
    minus = jnp.where(row < 3, -1.0, 0.0).astype(jnp.bfloat16)
    ones = jnp.ones((extra_rows, tokens), jnp.bfloat16)
    for head in range(head_count):
        for shift in range(x_count):
            chain = head * x_count + shift
            query_scratch[chain, :head_width] = query_refs[shift][
                head * head_width : (head + 1) * head_width
            ]
            query_scratch[chain, head_width:] = minus
            sum_scratch[chain] = jnp.zeros((deep, tokens), jnp.float32)
            peak_scratch[chain] = jnp.full((8, tokens), masked_score, jnp.float32)

    def one(chain, key_rows, value_rows, masked):
        scores = lax.dot_general(
            key_rows,
            query_scratch[chain],
            (((0,), (0,)), ((), ())),
            preferred_element_type=jnp.float32,
        )
        if masked:
            key_place = lax.broadcasted_iota(jnp.int32, scores.shape, 0)
            query_place = lax.broadcasted_iota(jnp.int32, scores.shape, 1)
            scores = jnp.where(key_place <= query_place, scores, masked_score)
        old_peak = peak_scratch[chain, :1]
        new_peak = jnp.maximum(old_peak, jnp.max(scores, axis=0, keepdims=True))
        weights = jnp.exp(scores - new_peak).astype(jnp.bfloat16)
        shrink = jnp.exp(old_peak - new_peak)
        sum_scratch[chain] = sum_scratch[chain] * shrink + jnp.dot(
            value_rows, weights, preferred_element_type=jnp.float32
        )
        peak_scratch[chain] = jnp.broadcast_to(new_peak, (8, tokens))

    def loaded(z_key, head):
        key_rows = kv_ref[z_key, head * deep : (head + 1) * deep]
        value_first = head_count * deep + head * head_width
        value_rows = kv_ref[z_key, value_first : value_first + head_width]
        return key_rows, jnp.concatenate([value_rows, ones], axis=0)

    def earlier(z_key, carry):
        for head in range(head_count):
            key_rows, value_rows = loaded(z_key, head)
            for shift in range(x_count):
                one(head * x_count + shift, key_rows, value_rows, False)
        return carry

    lax.fori_loop(0, z_place, earlier, 0)
    for head in range(head_count):
        key_rows, value_rows = loaded(z_place, head)
        one(head * x_count, key_rows, value_rows, True)
    for shift in range(1, x_count):

        @pl.when(x_place < shift)
        def _():
            for head in range(head_count):
                key_rows, value_rows = loaded(z_place, head)
                one(head * x_count + shift, key_rows, value_rows, False)

    for shift in range(x_count):
        target = lax.rem(x_place + x_count - shift, x_count)
        stats = jnp.zeros((extra_rows, tokens), jnp.float32)
        for head in range(head_count):
            chain = head * x_count + shift
            out_ref[target, head * head_width : (head + 1) * head_width] = sum_scratch[
                chain, :head_width
            ].astype(jnp.bfloat16)
            place = head * 6
            for full in (peak_scratch[chain, :1], sum_scratch[chain, head_width : head_width + 1]):
                for _ in range(3):
                    part = full.astype(jnp.bfloat16).astype(jnp.float32)
                    full = full - part
                    stats = jnp.where(row == place, part, stats)
                    place += 1
        out_ref[target, head_count * head_width :] = stats.astype(jnp.bfloat16)


def project_kernel(head_count, head_width, place_ref, parts_ref, weight_ref, mine_ref, other_ref, full_ref):
    x_count = parts_ref.shape[0]
    tp_half = mine_ref.shape[0]
    width = head_count * head_width
    core = place_ref[2]
    rows = []
    for head in range(head_count):
        peaks, totals = [], []
        for part in range(x_count):
            stats = parts_ref[part, width : width + extra_rows].astype(jnp.float32)
            base = head * 6
            peaks.append(stats[base : base + 1] + stats[base + 1 : base + 2] + stats[base + 2 : base + 3])
            totals.append(
                stats[base + 3 : base + 4] + stats[base + 4 : base + 5] + stats[base + 5 : base + 6]
            )
        top = functools.reduce(jnp.maximum, peaks)
        factors = [jnp.exp(peak - top) for peak in peaks]
        total = sum(factor * amount for factor, amount in zip(factors, totals))
        summed = sum(
            parts_ref[part, head * head_width : (head + 1) * head_width].astype(jnp.float32)
            * factors[part]
            for part in range(x_count)
        )
        rows.append((summed / total).astype(jnp.bfloat16))
    attended = jnp.concatenate(rows, axis=0)
    full_ref[...] = lax.dot_general(
        attended, weight_ref[...], (((0,), (0,)), ((), ())), preferred_element_type=jnp.float32
    ).astype(jnp.bfloat16)
    for block in range(tp_half):
        own = pl.multiple_of((block * 2 + core) * lane, lane)
        far = pl.multiple_of((block * 2 + 1 - core) * lane, lane)
        mine_ref[block] = full_ref[:, pl.ds(own, lane)]
        other_ref[block] = full_ref[:, pl.ds(far, lane)]


def expert_kernel(place_ref, rows_in_ref, gain_ref, *refs):
    sets = (len(refs) - 8) // 3
    gate_refs, up_refs, down_refs = refs[:sets], refs[sets : 2 * sets], refs[2 * sets : 3 * sets]
    out_ref, rows_ref, hidden_ref, full_ref, gates, ups, downs, sems = refs[3 * sets :]
    core = place_ref[2]
    blocks = rows_in_ref.shape[0]
    width = rows_ref.shape[1]
    units = gates.shape[2]
    copies = []
    for part in range(sets):
        for kind, (sources, target) in enumerate(((gate_refs, gates), (up_refs, ups), (down_refs, downs))):
            copy = pltpu.make_async_copy(sources[part], target.at[part], sems.at[kind, part])
            copy.start()
            copies.append(copy)
    squares = jnp.zeros(rows_in_ref.shape[2:], jnp.float32)
    for block in range(blocks):
        for side in range(2):
            values = rows_in_ref[block, side].astype(jnp.float32)
            squares = squares + values * values
    scale = lax.rsqrt(jnp.sum(squares, axis=1, keepdims=True) / width + norm_eps)
    for block in range(blocks):
        for side, at in ((0, core), (1, 1 - core)):
            index = block * 2 + at
            values = rows_in_ref[block, side].astype(jnp.float32) * scale * gain_ref[index]
            rows_ref[:, pl.ds(pl.multiple_of(index * lane, lane), lane)] = values.astype(jnp.bfloat16)
    for part in range(sets):
        copies[3 * part].wait()
        gate = jnp.dot(rows_ref[...], gates[part], preferred_element_type=jnp.float32)
        copies[3 * part + 1].wait()
        up = jnp.dot(rows_ref[...], ups[part], preferred_element_type=jnp.float32)
        hidden_ref[:, part * units : (part + 1) * units] = (
            gate / (1.0 + jnp.exp(-gate)) * up
        ).astype(jnp.bfloat16)
        copies[3 * part + 2].wait()
    full_ref[...] = jnp.dot(
        hidden_ref[...], downs[...].reshape(sets * units, width), preferred_element_type=jnp.float32
    ).astype(jnp.bfloat16)
    out_width = out_ref.shape[2]
    for block in range(blocks):
        out_ref[block] = full_ref[:, block * out_width : (block + 1) * out_width]


def shards(
    residual,
    queries,
    keys,
    values,
    forget_cache,
    out_weight,
    norm_gain,
    routes,
    route_weight,
    gate_weight,
    up_weight,
    down_weight,
):
    z_count, x_count, y_count = (lax.axis_size(axis) for axis in ("z", "x", "y"))
    sp_count = z_count * x_count
    token_count, local_width = residual.shape
    model_width = norm_gain.shape[0]
    head_count = forget_cache.shape[0]
    head_width = queries.shape[0] // head_count
    top_count = routes.shape[1]
    capacity = max(2, token_count * top_count * 5 // (4 * sp_count))
    slot_total = sp_count * capacity
    bf16, f32 = jnp.bfloat16, jnp.float32
    place = jnp.stack(
        [lax.axis_index("z"), lax.axis_index("x"), lax.axis_index("c"), lax.axis_index("y")]
    ).astype(jnp.int32)
    smem = pl.BlockSpec(memory_space=pltpu.SMEM)
    vmem = pl.BlockSpec(memory_space=pltpu.VMEM)

    gates = jnp.stack(split_three(forget_cache), axis=1)
    gates = jnp.pad(gates, ((0, 0), (0, extra_rows - 3), (0, 0)))
    key_rows = jnp.concatenate([keys.reshape(head_count, head_width, token_count), gates], axis=1)
    message = jnp.concatenate([key_rows.reshape(-1, token_count), values], axis=0)
    gathered = sent_to_all(message, "z")
    scaled = queries * jnp.asarray(head_width ** (-0.5), bf16)
    query_list = [scaled] + [
        lax.ppermute(scaled, "x", [(i, (i + shift) % x_count) for i in range(x_count)])
        for shift in range(1, x_count)
    ]
    slice_moves = []
    for y_from in range(y_count):
        slice_moves.append((2 * y_from, 2 * ((y_from - 1) % y_count)))
        slice_moves.append((2 * y_from + 1, 2 * ((y_from + 1) % y_count) + 1))
    own_set = (gate_weight[0], up_weight[0], down_weight[0])
    near_set = tuple(lax.ppermute(weight, TP, slice_moves) for weight in own_set)
    own_swapped = tuple(swapped(weight) for weight in own_set)
    near_swapped = tuple(swapped(weight) for weight in near_set)
    chains = head_count * x_count
    deep = head_width + extra_rows
    part_rows = head_count * head_width + extra_rows
    attend = pl.pallas_call(
        functools.partial(attend_kernel, head_count, head_width),
        out_shape=jax.ShapeDtypeStruct((x_count, part_rows, token_count), bf16),
        in_specs=[smem] + [vmem] * (1 + x_count),
        out_specs=vmem,
        scratch_shapes=[
            pltpu.VMEM((chains, deep, token_count), bf16),
            pltpu.VMEM((chains, deep, token_count), f32),
            pltpu.VMEM((chains, 8, token_count), f32),
        ],
        name="attend",
        interpret=INTERPRET,
    )
    parts = attend(place, gathered, *query_list)

    expert_ids = jnp.arange(sp_count, dtype=jnp.int32)
    chosen = routes[:, :, None] == expert_ids
    named = jnp.any(chosen, axis=1)
    token_ids = jnp.arange(token_count, dtype=jnp.int32)
    before = (token_ids[None, :] < token_ids[:, None]).astype(bf16)
    rank = jnp.dot(before, named.astype(bf16), preferred_element_type=f32).astype(jnp.int32)
    slot_ids = jnp.arange(capacity, dtype=jnp.int32)
    taken = (named.T[:, None, :] & (rank.T[:, None, :] == slot_ids[:, None])).astype(bf16)
    taken = taken.reshape(slot_total, token_count)
    share = jnp.sum(jnp.where(chosen, route_weight[:, :, None], 0.0), axis=1)
    share_first = lax.reduce_precision(share, 8, 7)
    share_rest = (share - share_first).astype(bf16)

    def spread(weights):
        return jnp.where(
            rank[:, :, None] == slot_ids, weights.astype(bf16)[:, :, None], jnp.zeros((), bf16)
        ).reshape(token_count, slot_total)

    give_first, give_rest = spread(share_first), spread(share_rest)

    received = lax.all_to_all(parts, "x", split_axis=0, concat_axis=0, tiled=True)
    half = jax.ShapeDtypeStruct((y_count, token_count, local_width), bf16)
    mine, other = pl.pallas_call(
        functools.partial(project_kernel, head_count, head_width),
        out_shape=(half, half),
        in_specs=[smem, vmem, vmem],
        out_specs=(vmem, vmem),
        scratch_shapes=[pltpu.VMEM((token_count, model_width), bf16)],
        name="project",
        interpret=INTERPRET,
    )(place, received, out_weight)
    paired = (mine.astype(f32) + swapped(other).astype(f32)).astype(bf16)
    pieces = lax.all_to_all(paired, "y", split_axis=0, concat_axis=0, tiled=True)
    pieces, own_swapped, near_set, near_swapped = lax.optimization_barrier(
        (pieces, own_swapped, near_set, near_swapped)
    )
    weight_sets = [own_set, own_swapped, near_set, near_swapped]
    head_sum = jnp.sum(pieces.astype(f32), axis=0)
    stream = (residual.astype(f32) + head_sum).astype(bf16)

    sent = jnp.dot(taken, stream, preferred_element_type=f32).astype(bf16)
    arrived = lax.all_to_all(
        sent.reshape(sp_count, capacity, local_width), SP, split_axis=0, concat_axis=0, tiled=True
    ).reshape(slot_total, local_width)
    quarter = slot_total // 4
    arrived = arrived.reshape(2, 2, quarter, local_width)
    core = place[2]
    mine = lax.dynamic_index_in_dim(arrived, core, 1, keepdims=False)
    other = lax.dynamic_index_in_dim(arrived, 1 - core, 1, keepdims=False)
    both = jnp.stack([mine, swapped(other)], axis=1)
    both = jnp.broadcast_to(both, (y_count // 2, *both.shape))
    rows = lax.all_to_all(
        both.reshape(y_count, 2, quarter, local_width), "y", split_axis=0, concat_axis=0, tiled=True
    )
    weights = [kind[part] for kind in zip(*weight_sets) for part in range(len(weight_sets))]
    sets = len(weight_sets)
    hidden_units = gate_weight.shape[2]
    any_space = pl.BlockSpec(memory_space=pl.ANY)
    out_rows = pl.pallas_call(
        expert_kernel,
        out_shape=jax.ShapeDtypeStruct((y_count, quarter, 2 * local_width), bf16),
        in_specs=[smem, vmem, vmem] + [any_space] * (3 * sets),
        out_specs=vmem,
        scratch_shapes=[
            pltpu.VMEM((quarter, model_width), bf16),
            pltpu.VMEM((quarter, sets * hidden_units), bf16),
            pltpu.VMEM((quarter, model_width), bf16),
            pltpu.VMEM((sets, model_width, hidden_units), bf16),
            pltpu.VMEM((sets, model_width, hidden_units), bf16),
            pltpu.VMEM((sets, hidden_units, model_width), bf16),
            pltpu.SemaphoreType.DMA((3, sets)),
        ],
        name="expert",
        interpret=INTERPRET,
    )(place, rows, norm_gain.reshape(2 * y_count, 1, lane), *weights)
    pieces = lax.all_to_all(out_rows, "y", split_axis=0, concat_axis=0, tiled=True)
    summed = jnp.sum(
        pieces.reshape(y_count // 2, 2, quarter, 2, local_width).astype(f32), axis=0
    ).astype(bf16)
    mine = lax.dynamic_index_in_dim(summed, core, 2, keepdims=False)
    got = swapped(lax.dynamic_index_in_dim(summed, 1 - core, 2, keepdims=False))
    first = core == 0
    expert_out = jnp.stack([jnp.where(first, mine, got), jnp.where(first, got, mine)], axis=1)
    back = lax.all_to_all(
        expert_out.reshape(sp_count, capacity, local_width), SP, split_axis=0, concat_axis=0, tiled=True
    ).reshape(slot_total, local_width)
    mixture = jnp.dot(give_first, back, preferred_element_type=f32) + jnp.dot(
        give_rest, back, preferred_element_type=f32
    )
    return (stream.astype(f32) + mixture).astype(bf16)


def solution(mesh):
    sp_count, tp_count = mesh.shape["sp"], mesh.shape["tp"]
    x_count = 4 if sp_count % 8 == 0 else 2
    finer = Mesh(
        mesh.devices.reshape(sp_count // x_count, x_count, tp_count // 2, 2), ("z", "x", "y", "c")
    )
    in_specs = (
        P(SP, TP),
        P(TP, SP),
        P(TP, SP),
        P(TP, SP),
        P(TP, SP),
        P(TP, None),
        P(),
        P(SP, None),
        P(SP, None),
        P(SP, None, TP),
        P(SP, None, TP),
        P(SP, TP, None),
    )
    return jax.shard_map(
        shards, mesh=finer, in_specs=in_specs, out_specs=P(SP, TP), check_vma=False
    )
```

```python
import functools

import jax
import jax.numpy as jnp
from jax import lax
from jax.experimental import pallas as pl
from jax.experimental.pallas import tpu as pltpu
from jax.sharding import Mesh
from jax.sharding import PartitionSpec as P


SP = ("z", "x")
TP = ("y", "c")
INTERPRET = False

norm_eps = 1e-06
masked_score = -1e30
extra_rows = 16
lane = 128


def swapped(shard):
    return lax.ppermute(shard, "c", [(0, 1), (1, 0)])


def three_parts(full):
    parts = []
    for _ in range(3):
        part = full.astype(jnp.bfloat16).astype(jnp.float32)
        full = full - part
        parts.append(part)
    return parts


def pack_kernel(head_width, keys_ref, values_ref, gates_ref, queries_ref, out_ref, query_ref):
    tokens = keys_ref.shape[1]
    head_count = gates_ref.shape[0]
    row = lax.broadcasted_iota(jnp.int32, (extra_rows, tokens), 0)
    pieces = []
    for head in range(head_count):
        gates = jnp.zeros((extra_rows, tokens), jnp.float32)
        for place, part in enumerate(three_parts(gates_ref[head : head + 1])):
            gates = jnp.where(row == place, part, gates)
        pieces += [keys_ref[head * head_width : (head + 1) * head_width], gates.astype(jnp.bfloat16)]
    message = jnp.concatenate(pieces + [values_ref[...]], axis=0)
    for copy in range(out_ref.shape[0]):
        out_ref[copy] = message
    query_ref[...] = queries_ref[...] * jnp.asarray(head_width ** (-0.5), jnp.bfloat16)


def attend_kernel(head_count, head_width, place_ref, kv_ref, *refs):
    out_ref, query_scratch, key_scratch, value_scratch = refs[-4:]
    query_refs = refs[:-4]
    tokens = kv_ref.shape[2]
    z_count, x_count = kv_ref.shape[0], len(query_refs)
    deep = head_width + extra_rows
    z_place, x_place = place_ref[0], place_ref[1]
    row = lax.broadcasted_iota(jnp.int32, (extra_rows, tokens), 0)
    minus = jnp.where(row < 3, -1.0, 0.0).astype(jnp.bfloat16)
    ones = jnp.ones((extra_rows, tokens), jnp.bfloat16)
    for head in range(head_count):
        rows = slice(head * head_width, (head + 1) * head_width)
        for shift in range(x_count):
            target = lax.rem(x_place + x_count - shift, x_count)
            columns = pl.ds(pl.multiple_of(target * tokens, tokens), tokens)
            query_scratch[head, :head_width, columns] = query_refs[shift][rows]
            query_scratch[head, head_width:, columns] = minus
        for block in range(z_count):
            columns = slice(block * tokens, (block + 1) * tokens)
            key_scratch[head, :, columns] = kv_ref[block, head * deep : (head + 1) * deep]
            first = head_count * deep + head * head_width
            value_scratch[head, :head_width, columns] = kv_ref[block, first : first + head_width]
            value_scratch[head, head_width:, columns] = ones
    wide = 2 * tokens if x_count % 2 == 0 else tokens
    for head in range(head_count):
        rows = slice(head * head_width, (head + 1) * head_width)
        for first in range(0, x_count * tokens, wide):
            scores = lax.dot_general(
                key_scratch[head],
                query_scratch[head, :, first : first + wide],
                (((0,), (0,)), ((), ())),
                preferred_element_type=jnp.float32,
            )
            key_row = lax.broadcasted_iota(jnp.int32, scores.shape, 0)
            key_place = key_row // tokens * (x_count * tokens) + key_row % tokens
            key_place = key_place + x_place * tokens
            query_place = lax.broadcasted_iota(jnp.int32, scores.shape, 1)
            query_place = query_place + (z_place * (x_count * tokens) + first)
            scores = jnp.where(key_place <= query_place, scores, 2 * masked_score)
            peak = jnp.maximum(jnp.max(scores, axis=0, keepdims=True), masked_score)
            weights = jnp.exp(scores - peak).astype(jnp.bfloat16)
            summed = jnp.dot(value_scratch[head], weights, preferred_element_type=jnp.float32)
            for block in range(first // tokens, (first + wide) // tokens):
                columns = slice(block * tokens - first, (block + 1) * tokens - first)
                out_ref[block, rows] = summed[:head_width, columns].astype(jnp.bfloat16)
                stats = jnp.zeros((extra_rows, tokens), jnp.float32)
                total = summed[head_width : head_width + 1, columns]
                for place, part in enumerate(three_parts(peak[:, columns]) + three_parts(total)):
                    stats = jnp.where(row == place, part, stats)
                base = head_count * head_width + head * extra_rows
                out_ref[block, base : base + extra_rows] = stats.astype(jnp.bfloat16)


def project_kernel(head_count, head_width, place_ref, parts_ref, weight_ref, mine_ref, other_ref, full_ref):
    x_count = parts_ref.shape[0]
    tp_half = mine_ref.shape[0]
    core = place_ref[2]
    rows = []
    for head in range(head_count):
        peaks, totals = [], []
        base = head_count * head_width + head * extra_rows
        for part in range(x_count):
            stats = parts_ref[part, base : base + extra_rows].astype(jnp.float32)
            peaks.append(stats[0:1] + stats[1:2] + stats[2:3])
            totals.append(stats[3:4] + stats[4:5] + stats[5:6])
        top = functools.reduce(jnp.maximum, peaks)
        factors = [jnp.exp(peak - top) for peak in peaks]
        total = sum(factor * amount for factor, amount in zip(factors, totals))
        summed = sum(
            parts_ref[part, head * head_width : (head + 1) * head_width].astype(jnp.float32)
            * factors[part]
            for part in range(x_count)
        )
        rows.append((summed / total).astype(jnp.bfloat16))
    attended = jnp.concatenate(rows, axis=0)
    full_ref[...] = lax.dot_general(
        attended, weight_ref[...], (((0,), (0,)), ((), ())), preferred_element_type=jnp.float32
    ).astype(jnp.bfloat16)
    for block in range(tp_half):
        own = pl.multiple_of((block * 2 + core) * lane, lane)
        far = pl.multiple_of((block * 2 + 1 - core) * lane, lane)
        mine_ref[block] = full_ref[:, pl.ds(own, lane)]
        other_ref[block] = full_ref[:, pl.ds(far, lane)]


def expert_kernel(place_ref, rows_in_ref, gain_ref, *refs):
    sets = (len(refs) - 8) // 3
    gate_refs, up_refs, down_refs = refs[:sets], refs[sets : 2 * sets], refs[2 * sets : 3 * sets]
    out_ref, rows_ref, hidden_ref, full_ref, gates, ups, downs, sems = refs[3 * sets :]
    core = place_ref[2]
    blocks = rows_in_ref.shape[0]
    width = rows_ref.shape[1]
    units = gates.shape[2]
    copies = []
    for part in range(sets):
        for kind, (sources, target) in enumerate(((gate_refs, gates), (up_refs, ups), (down_refs, downs))):
            copy = pltpu.make_async_copy(sources[part], target.at[part], sems.at[kind, part])
            copy.start()
            copies.append(copy)
    squares = jnp.zeros(rows_in_ref.shape[2:], jnp.float32)
    for block in range(blocks):
        for side in range(2):
            values = rows_in_ref[block, side].astype(jnp.float32)
            squares = squares + values * values
    scale = lax.rsqrt(jnp.sum(squares, axis=1, keepdims=True) / width + norm_eps)
    for block in range(blocks):
        for side, at in ((0, core), (1, 1 - core)):
            index = block * 2 + at
            values = rows_in_ref[block, side].astype(jnp.float32) * scale * gain_ref[index]
            rows_ref[:, pl.ds(pl.multiple_of(index * lane, lane), lane)] = values.astype(jnp.bfloat16)
    for part in range(sets):
        copies[3 * part].wait()
        gate = jnp.dot(rows_ref[...], gates[part], preferred_element_type=jnp.float32)
        copies[3 * part + 1].wait()
        up = jnp.dot(rows_ref[...], ups[part], preferred_element_type=jnp.float32)
        hidden_ref[:, part * units : (part + 1) * units] = (
            gate / (1.0 + jnp.exp(-gate)) * up
        ).astype(jnp.bfloat16)
        copies[3 * part + 2].wait()
    full_ref[...] = jnp.dot(
        hidden_ref[...], downs[...].reshape(sets * units, width), preferred_element_type=jnp.float32
    ).astype(jnp.bfloat16)
    out_width = out_ref.shape[2]
    for block in range(blocks):
        out_ref[block] = full_ref[:, block * out_width : (block + 1) * out_width]


def shards(
    residual,
    queries,
    keys,
    values,
    forget_cache,
    out_weight,
    norm_gain,
    routes,
    route_weight,
    gate_weight,
    up_weight,
    down_weight,
):
    z_count, x_count, y_count = (lax.axis_size(axis) for axis in ("z", "x", "y"))
    sp_count = z_count * x_count
    token_count, local_width = residual.shape
    model_width = norm_gain.shape[0]
    head_count = forget_cache.shape[0]
    head_width = queries.shape[0] // head_count
    top_count = routes.shape[1]
    capacity = max(2, token_count * top_count * 5 // (4 * sp_count))
    slot_total = sp_count * capacity
    bf16, f32 = jnp.bfloat16, jnp.float32
    place = jnp.stack(
        [lax.axis_index("z"), lax.axis_index("x"), lax.axis_index("c"), lax.axis_index("y")]
    ).astype(jnp.int32)
    smem = pl.BlockSpec(memory_space=pltpu.SMEM)
    vmem = pl.BlockSpec(memory_space=pltpu.VMEM)

    deep = head_width + extra_rows
    message_rows = head_count * (deep + head_width)
    message, scaled = pl.pallas_call(
        functools.partial(pack_kernel, head_width),
        out_shape=(
            jax.ShapeDtypeStruct((z_count, message_rows, token_count), bf16),
            jax.ShapeDtypeStruct(queries.shape, bf16),
        ),
        in_specs=[vmem] * 4,
        out_specs=(vmem, vmem),
        name="pack",
        interpret=INTERPRET,
    )(keys, values, forget_cache, queries)
    gathered = lax.all_to_all(message, "z", split_axis=0, concat_axis=0, tiled=True)
    query_list = [scaled] + [
        lax.ppermute(scaled, "x", [(i, (i + shift) % x_count) for i in range(x_count)])
        for shift in range(1, x_count)
    ]
    slice_moves = []
    for y_from in range(y_count):
        slice_moves.append((2 * y_from, 2 * ((y_from - 1) % y_count)))
        slice_moves.append((2 * y_from + 1, 2 * ((y_from + 1) % y_count) + 1))
    own_set = (gate_weight[0], up_weight[0], down_weight[0])
    near_set = tuple(lax.ppermute(weight, TP, slice_moves) for weight in own_set)
    own_swapped = tuple(swapped(weight) for weight in own_set)
    attend = pl.pallas_call(
        functools.partial(attend_kernel, head_count, head_width),
        out_shape=jax.ShapeDtypeStruct((x_count, head_count * deep, token_count), bf16),
        in_specs=[smem] + [vmem] * (1 + x_count),
        out_specs=vmem,
        scratch_shapes=[
            pltpu.VMEM((head_count, deep, x_count * token_count), bf16),
            pltpu.VMEM((head_count, deep, z_count * token_count), bf16),
            pltpu.VMEM((head_count, deep, z_count * token_count), bf16),
        ],
        name="attend",
        interpret=INTERPRET,
    )
    parts = attend(place, gathered, *query_list)
    received = lax.all_to_all(parts, "x", split_axis=0, concat_axis=0, tiled=True)

    expert_ids = jnp.arange(sp_count, dtype=jnp.int32)
    chosen = routes[:, :, None] == expert_ids
    named = jnp.any(chosen, axis=1)
    token_ids = jnp.arange(token_count, dtype=jnp.int32)
    before = (token_ids[None, :] < token_ids[:, None]).astype(bf16)
    rank = jnp.dot(before, named.astype(bf16), preferred_element_type=f32).astype(jnp.int32)
    slot_ids = jnp.arange(capacity, dtype=jnp.int32)
    taken = (named.T[:, None, :] & (rank.T[:, None, :] == slot_ids[:, None])).astype(bf16)
    taken = taken.reshape(slot_total, token_count)
    share = jnp.sum(jnp.where(chosen, route_weight[:, :, None], 0.0), axis=1)
    share_first = lax.reduce_precision(share, 8, 7)
    share_rest = (share - share_first).astype(bf16)

    def spread(weights):
        return jnp.where(
            rank[:, :, None] == slot_ids, weights.astype(bf16)[:, :, None], jnp.zeros((), bf16)
        ).reshape(token_count, slot_total)

    give_first, give_rest = spread(share_first), spread(share_rest)

    half = jax.ShapeDtypeStruct((y_count, token_count, local_width), bf16)
    mine, other = pl.pallas_call(
        functools.partial(project_kernel, head_count, head_width),
        out_shape=(half, half),
        in_specs=[smem, vmem, vmem],
        out_specs=(vmem, vmem),
        scratch_shapes=[pltpu.VMEM((token_count, model_width), bf16)],
        name="project",
        interpret=INTERPRET,
    )(place, received, out_weight)
    paired = (mine.astype(f32) + swapped(other).astype(f32)).astype(bf16)
    pieces = lax.all_to_all(paired, "y", split_axis=0, concat_axis=0, tiled=True)
    pieces, own_swapped, near_set = lax.optimization_barrier((pieces, own_swapped, near_set))
    near_swapped = tuple(swapped(weight) for weight in near_set)
    head_sum = jnp.sum(pieces.astype(f32), axis=0)
    stream = (residual.astype(f32) + head_sum).astype(bf16)

    sent = jnp.dot(taken, stream, preferred_element_type=f32).astype(bf16)
    arrived = lax.all_to_all(
        sent.reshape(sp_count, capacity, local_width), SP, split_axis=0, concat_axis=0, tiled=True
    )
    arrived, near_swapped = lax.optimization_barrier((arrived, near_swapped))
    weight_sets = [own_set, own_swapped, near_set, near_swapped]
    quarter = slot_total // 4
    arrived = arrived.reshape(2, 2, quarter, local_width)
    core = place[2]
    mine = lax.dynamic_index_in_dim(arrived, core, 1, keepdims=False)
    other = lax.dynamic_index_in_dim(arrived, 1 - core, 1, keepdims=False)
    both = jnp.stack([mine, swapped(other)], axis=1)
    both = jnp.broadcast_to(both, (y_count // 2, *both.shape))
    rows = lax.all_to_all(
        both.reshape(y_count, 2, quarter, local_width), "y", split_axis=0, concat_axis=0, tiled=True
    )
    weights = [kind[part] for kind in zip(*weight_sets) for part in range(len(weight_sets))]
    sets = len(weight_sets)
    hidden_units = gate_weight.shape[2]
    any_space = pl.BlockSpec(memory_space=pl.ANY)
    out_rows = pl.pallas_call(
        expert_kernel,
        out_shape=jax.ShapeDtypeStruct((y_count, quarter, 2 * local_width), bf16),
        in_specs=[smem, vmem, vmem] + [any_space] * (3 * sets),
        out_specs=vmem,
        scratch_shapes=[
            pltpu.VMEM((quarter, model_width), bf16),
            pltpu.VMEM((quarter, sets * hidden_units), bf16),
            pltpu.VMEM((quarter, model_width), bf16),
            pltpu.VMEM((sets, model_width, hidden_units), bf16),
            pltpu.VMEM((sets, model_width, hidden_units), bf16),
            pltpu.VMEM((sets, hidden_units, model_width), bf16),
            pltpu.SemaphoreType.DMA((3, sets)),
        ],
        name="expert",
        interpret=INTERPRET,
    )(place, rows, norm_gain.reshape(2 * y_count, 1, lane), *weights)
    pieces = lax.all_to_all(out_rows, "y", split_axis=0, concat_axis=0, tiled=True)
    summed = jnp.sum(
        pieces.reshape(y_count // 2, 2, quarter, 2, local_width).astype(f32), axis=0
    ).astype(bf16)
    mine = lax.dynamic_index_in_dim(summed, core, 2, keepdims=False)
    got = swapped(lax.dynamic_index_in_dim(summed, 1 - core, 2, keepdims=False))
    first = core == 0
    expert_out = jnp.stack([jnp.where(first, mine, got), jnp.where(first, got, mine)], axis=1)
    back = lax.all_to_all(
        expert_out.reshape(sp_count, capacity, local_width), SP, split_axis=0, concat_axis=0, tiled=True
    ).reshape(slot_total, local_width)
    mixture = jnp.dot(give_first, back, preferred_element_type=f32) + jnp.dot(
        give_rest, back, preferred_element_type=f32
    )
    return (stream.astype(f32) + mixture).astype(bf16)


def solution(mesh):
    sp_count, tp_count = mesh.shape["sp"], mesh.shape["tp"]
    x_count = 4 if sp_count % 8 == 0 else 2
    finer = Mesh(
        mesh.devices.reshape(sp_count // x_count, x_count, tp_count // 2, 2), ("z", "x", "y", "c")
    )
    in_specs = (
        P(SP, TP),
        P(TP, SP),
        P(TP, SP),
        P(TP, SP),
        P(TP, SP),
        P(TP, None),
        P(),
        P(SP, None),
        P(SP, None),
        P(SP, None, TP),
        P(SP, None, TP),
        P(SP, TP, None),
    )
    return jax.shard_map(
        shards, mesh=finer, in_specs=in_specs, out_specs=P(SP, TP), check_vma=False
    )
```

```python
import functools

import jax
import jax.numpy as jnp
from jax import lax
from jax.experimental import pallas as pl
from jax.experimental.pallas import tpu as pltpu
from jax.sharding import Mesh
from jax.sharding import PartitionSpec as P


SP = ("z", "x")
TP = ("y", "c")
INTERPRET = False

norm_eps = 1e-06
masked_score = -1e30
extra_rows = 16
lane = 128


def swapped(shard):
    return lax.ppermute(shard, "c", [(0, 1), (1, 0)])


def three_parts(full):
    parts = []
    for _ in range(3):
        part = full.astype(jnp.bfloat16).astype(jnp.float32)
        full = full - part
        parts.append(part)
    return parts


def pack_kernel(head_width, keys_ref, values_ref, gates_ref, queries_ref, out_ref, query_ref):
    tokens = keys_ref.shape[1]
    head_count = gates_ref.shape[0]
    row = lax.broadcasted_iota(jnp.int32, (extra_rows, tokens), 0)
    pieces = []
    for head in range(head_count):
        gates = jnp.zeros((extra_rows, tokens), jnp.float32)
        for place, part in enumerate(three_parts(gates_ref[head : head + 1])):
            gates = jnp.where(row == place, part, gates)
        pieces += [keys_ref[head * head_width : (head + 1) * head_width], gates.astype(jnp.bfloat16)]
    message = jnp.concatenate(pieces + [values_ref[...]], axis=0)
    for copy in range(out_ref.shape[0]):
        out_ref[copy] = message
    query_ref[...] = queries_ref[...] * jnp.asarray(head_width ** (-0.5), jnp.bfloat16)


def attend_kernel(head_count, head_width, place_ref, kv_ref, *refs):
    out_ref, query_scratch, key_scratch, value_scratch = refs[-4:]
    query_refs = refs[:-4]
    tokens = kv_ref.shape[2]
    z_count, x_count = kv_ref.shape[0], len(query_refs)
    deep = head_width + extra_rows
    z_place, x_place = place_ref[0], place_ref[1]
    row = lax.broadcasted_iota(jnp.int32, (extra_rows, tokens), 0)
    minus = jnp.where(row < 3, -1.0, 0.0).astype(jnp.bfloat16)
    ones = jnp.ones((extra_rows, tokens), jnp.bfloat16)
    for head in range(head_count):
        rows = slice(head * head_width, (head + 1) * head_width)
        for shift in range(x_count):
            target = lax.rem(x_place + x_count - shift, x_count)
            columns = pl.ds(pl.multiple_of(target * tokens, tokens), tokens)
            query_scratch[head, :head_width, columns] = query_refs[shift][rows]
            query_scratch[head, head_width:, columns] = minus
        for block in range(z_count):
            columns = slice(block * tokens, (block + 1) * tokens)
            key_scratch[head, :, columns] = kv_ref[block, head * deep : (head + 1) * deep]
            first = head_count * deep + head * head_width
            value_scratch[head, :head_width, columns] = kv_ref[block, first : first + head_width]
            value_scratch[head, head_width:, columns] = ones
    wide = 2 * tokens if x_count % 2 == 0 else tokens
    for head in range(head_count):
        rows = slice(head * head_width, (head + 1) * head_width)
        for first in range(0, x_count * tokens, wide):
            scores = lax.dot_general(
                key_scratch[head],
                query_scratch[head, :, first : first + wide],
                (((0,), (0,)), ((), ())),
                preferred_element_type=jnp.float32,
            )
            key_row = lax.broadcasted_iota(jnp.int32, scores.shape, 0)
            key_place = key_row // tokens * (x_count * tokens) + key_row % tokens
            key_place = key_place + x_place * tokens
            query_place = lax.broadcasted_iota(jnp.int32, scores.shape, 1)
            query_place = query_place + (z_place * (x_count * tokens) + first)
            scores = jnp.where(key_place <= query_place, scores, 2 * masked_score)
            peak = jnp.maximum(jnp.max(scores, axis=0, keepdims=True), masked_score)
            weights = jnp.exp(scores - peak).astype(jnp.bfloat16)
            summed = jnp.dot(value_scratch[head], weights, preferred_element_type=jnp.float32)
            for block in range(first // tokens, (first + wide) // tokens):
                columns = slice(block * tokens - first, (block + 1) * tokens - first)
                out_ref[block, rows] = summed[:head_width, columns].astype(jnp.bfloat16)
                stats = jnp.zeros((extra_rows, tokens), jnp.float32)
                total = summed[head_width : head_width + 1, columns]
                for place, part in enumerate(three_parts(peak[:, columns]) + three_parts(total)):
                    stats = jnp.where(row == place, part, stats)
                base = head_count * head_width + head * extra_rows
                out_ref[block, base : base + extra_rows] = stats.astype(jnp.bfloat16)


def project_kernel(head_count, head_width, place_ref, parts_ref, weight_ref, mine_ref, other_ref, full_ref):
    x_count = parts_ref.shape[0]
    tp_half = mine_ref.shape[0]
    core = place_ref[2]
    rows = []
    for head in range(head_count):
        peaks, totals = [], []
        base = head_count * head_width + head * extra_rows
        for part in range(x_count):
            stats = parts_ref[part, base : base + extra_rows].astype(jnp.float32)
            peaks.append(stats[0:1] + stats[1:2] + stats[2:3])
            totals.append(stats[3:4] + stats[4:5] + stats[5:6])
        top = functools.reduce(jnp.maximum, peaks)
        factors = [jnp.exp(peak - top) for peak in peaks]
        total = sum(factor * amount for factor, amount in zip(factors, totals))
        summed = sum(
            parts_ref[part, head * head_width : (head + 1) * head_width].astype(jnp.float32)
            * factors[part]
            for part in range(x_count)
        )
        rows.append((summed / total).astype(jnp.bfloat16))
    attended = jnp.concatenate(rows, axis=0)
    full_ref[...] = lax.dot_general(
        attended, weight_ref[...], (((0,), (0,)), ((), ())), preferred_element_type=jnp.float32
    ).astype(jnp.bfloat16)
    for block in range(tp_half):
        own = pl.multiple_of((block * 2 + core) * lane, lane)
        far = pl.multiple_of((block * 2 + 1 - core) * lane, lane)
        mine_ref[block] = full_ref[:, pl.ds(own, lane)]
        other_ref[block] = full_ref[:, pl.ds(far, lane)]


def pack_weights_kernel(gate_ref, up_ref, down_ref, out_ref, sems):
    units = gate_ref.shape[1]
    copies = [
        pltpu.make_async_copy(gate_ref, out_ref.at[0], sems.at[0]),
        pltpu.make_async_copy(up_ref, out_ref.at[1], sems.at[1]),
    ]
    for block in range(down_ref.shape[1] // units):
        columns = pl.ds(block * units, units)
        copies.append(
            pltpu.make_async_copy(
                down_ref.at[:, columns], out_ref.at[2, columns, :], sems.at[2 + block]
            )
        )
    for copy in copies:
        copy.start()
    for copy in copies:
        copy.wait()


def expert_kernel(rows_in_ref, gain_ref, *refs):
    sets = len(refs) - 8
    set_refs = refs[:sets]
    out_ref, rows_ref, hidden_ref, full_ref, gates, ups, downs, sems = refs[sets:]
    blocks = rows_in_ref.shape[0]
    width = rows_ref.shape[1]
    units = gates.shape[2]
    gate_copies, up_copies, down_copies = [], [], []
    for part in range(sets):
        gate_copies.append(
            pltpu.make_async_copy(set_refs[part].at[0], gates.at[part], sems.at[part, 0])
        )
        up_copies.append(pltpu.make_async_copy(set_refs[part].at[1], ups.at[part], sems.at[part, 1]))
        gate_copies[part].start()
        up_copies[part].start()
    for part in range(sets):
        for block in range(width // units):
            columns = pl.ds(block * units, units)
            down_copies.append(
                pltpu.make_async_copy(
                    set_refs[part].at[2, columns, :], downs.at[part, :, columns], sems.at[part, 2 + block]
                )
            )
            down_copies[-1].start()
    squares = jnp.zeros(rows_in_ref.shape[1:], jnp.float32)
    for block in range(blocks):
        values = rows_in_ref[block].astype(jnp.float32)
        squares = squares + values * values
    scale = lax.rsqrt(jnp.sum(squares, axis=1, keepdims=True) / width + norm_eps)
    for block in range(blocks):
        values = rows_in_ref[block].astype(jnp.float32) * scale * gain_ref[block]
        rows_ref[:, block * lane : (block + 1) * lane] = values.astype(jnp.bfloat16)
    for part in range(sets):
        gate_copies[part].wait()
        gate = jnp.dot(rows_ref[...], gates[part], preferred_element_type=jnp.float32)
        up_copies[part].wait()
        up = jnp.dot(rows_ref[...], ups[part], preferred_element_type=jnp.float32)
        hidden_ref[:, part * units : (part + 1) * units] = (
            gate / (1.0 + jnp.exp(-gate)) * up
        ).astype(jnp.bfloat16)
    for copy in down_copies:
        copy.wait()
    full_ref[...] = jnp.dot(
        hidden_ref[...], downs[...].reshape(sets * units, width), preferred_element_type=jnp.float32
    ).astype(jnp.bfloat16)
    for block in range(blocks):
        out_ref[block] = full_ref[:, block * lane : (block + 1) * lane]


def shards(
    residual,
    queries,
    keys,
    values,
    forget_cache,
    out_weight,
    norm_gain,
    routes,
    route_weight,
    gate_weight,
    up_weight,
    down_weight,
):
    z_count, x_count, y_count = (lax.axis_size(axis) for axis in ("z", "x", "y"))
    sp_count = z_count * x_count
    token_count, local_width = residual.shape
    model_width = norm_gain.shape[0]
    head_count = forget_cache.shape[0]
    head_width = queries.shape[0] // head_count
    top_count = routes.shape[1]
    capacity = max(2, token_count * top_count * 5 // (4 * sp_count))
    slot_total = sp_count * capacity
    bf16, f32 = jnp.bfloat16, jnp.float32
    place = jnp.stack(
        [lax.axis_index("z"), lax.axis_index("x"), lax.axis_index("c"), lax.axis_index("y")]
    ).astype(jnp.int32)
    smem = pl.BlockSpec(memory_space=pltpu.SMEM)
    vmem = pl.BlockSpec(memory_space=pltpu.VMEM)

    deep = head_width + extra_rows
    message_rows = head_count * (deep + head_width)
    message, scaled = pl.pallas_call(
        functools.partial(pack_kernel, head_width),
        out_shape=(
            jax.ShapeDtypeStruct((z_count, message_rows, token_count), bf16),
            jax.ShapeDtypeStruct(queries.shape, bf16),
        ),
        in_specs=[vmem] * 4,
        out_specs=(vmem, vmem),
        name="pack",
        interpret=INTERPRET,
    )(keys, values, forget_cache, queries)
    gathered = lax.all_to_all(message, "z", split_axis=0, concat_axis=0, tiled=True)
    query_list = [scaled] + [
        lax.ppermute(scaled, "x", [(i, (i + shift) % x_count) for i in range(x_count)])
        for shift in range(1, x_count)
    ]
    slice_moves = []
    for y_from in range(y_count):
        slice_moves.append((2 * y_from, 2 * ((y_from - 1) % y_count)))
        slice_moves.append((2 * y_from + 1, 2 * ((y_from + 1) % y_count) + 1))
    hidden_units = gate_weight.shape[2]
    any_space = pl.BlockSpec(memory_space=pl.ANY)
    down_blocks = model_width // hidden_units
    own_set = pl.pallas_call(
        pack_weights_kernel,
        out_shape=jax.ShapeDtypeStruct((3, model_width, hidden_units), bf16),
        in_specs=[any_space] * 3,
        out_specs=any_space,
        scratch_shapes=[pltpu.SemaphoreType.DMA((2 + down_blocks,))],
        name="pack_weights",
        interpret=INTERPRET,
    )(gate_weight[0], up_weight[0], down_weight[0])
    near_set = lax.ppermute(own_set, TP, slice_moves)
    own_swapped = swapped(own_set)
    near_swapped = swapped(near_set)
    attend = pl.pallas_call(
        functools.partial(attend_kernel, head_count, head_width),
        out_shape=jax.ShapeDtypeStruct((x_count, head_count * deep, token_count), bf16),
        in_specs=[smem] + [vmem] * (1 + x_count),
        out_specs=vmem,
        scratch_shapes=[
            pltpu.VMEM((head_count, deep, x_count * token_count), bf16),
            pltpu.VMEM((head_count, deep, z_count * token_count), bf16),
            pltpu.VMEM((head_count, deep, z_count * token_count), bf16),
        ],
        name="attend",
        interpret=INTERPRET,
    )
    parts = attend(place, gathered, *query_list)
    received = lax.all_to_all(parts, "x", split_axis=0, concat_axis=0, tiled=True)

    expert_ids = jnp.arange(sp_count, dtype=jnp.int32)
    chosen = routes[:, :, None] == expert_ids
    named = jnp.any(chosen, axis=1)
    token_ids = jnp.arange(token_count, dtype=jnp.int32)
    before = (token_ids[None, :] < token_ids[:, None]).astype(bf16)
    rank = jnp.dot(before, named.astype(bf16), preferred_element_type=f32).astype(jnp.int32)
    slot_ids = jnp.arange(capacity, dtype=jnp.int32)
    taken = (named.T[:, None, :] & (rank.T[:, None, :] == slot_ids[:, None])).astype(bf16)
    taken = taken.reshape(slot_total, token_count)
    share = jnp.sum(jnp.where(chosen, route_weight[:, :, None], 0.0), axis=1)
    share_first = lax.reduce_precision(share, 8, 7)
    share_rest = (share - share_first).astype(bf16)

    def spread(weights):
        return jnp.where(
            rank[:, :, None] == slot_ids, weights.astype(bf16)[:, :, None], jnp.zeros((), bf16)
        ).reshape(token_count, slot_total)

    give_first, give_rest = spread(share_first), spread(share_rest)

    half = jax.ShapeDtypeStruct((y_count, token_count, local_width), bf16)
    mine, other = pl.pallas_call(
        functools.partial(project_kernel, head_count, head_width),
        out_shape=(half, half),
        in_specs=[smem, vmem, vmem],
        out_specs=(vmem, vmem),
        scratch_shapes=[pltpu.VMEM((token_count, model_width), bf16)],
        name="project",
        interpret=INTERPRET,
    )(place, received, out_weight)
    paired = (mine.astype(f32) + swapped(other).astype(f32)).astype(bf16)
    pieces = lax.all_to_all(paired, "y", split_axis=0, concat_axis=0, tiled=True)
    pieces, own_swapped, near_set, near_swapped = lax.optimization_barrier(
        (pieces, own_swapped, near_set, near_swapped)
    )
    weight_sets = [own_set, own_swapped, near_set, near_swapped]
    head_sum = jnp.sum(pieces.astype(f32), axis=0)
    stream = (residual.astype(f32) + head_sum).astype(bf16)

    sent = jnp.dot(taken, stream, preferred_element_type=f32).astype(bf16)
    arrived = lax.all_to_all(
        sent.reshape(sp_count, capacity, local_width), SP, split_axis=0, concat_axis=0, tiled=True
    )
    quarter = slot_total // 4
    arrived = arrived.reshape(4, quarter, local_width)
    copies = jnp.broadcast_to(arrived, (y_count // 2, *arrived.shape))
    rows = lax.all_to_all(
        copies.reshape(2 * y_count, quarter, local_width), TP, split_axis=0, concat_axis=0, tiled=True
    )
    sets = len(weight_sets)
    out_rows = pl.pallas_call(
        expert_kernel,
        out_shape=jax.ShapeDtypeStruct((2 * y_count, quarter, local_width), bf16),
        in_specs=[vmem, vmem] + [any_space] * sets,
        out_specs=vmem,
        scratch_shapes=[
            pltpu.VMEM((quarter, model_width), bf16),
            pltpu.VMEM((quarter, sets * hidden_units), bf16),
            pltpu.VMEM((quarter, model_width), bf16),
            pltpu.VMEM((sets, model_width, hidden_units), bf16),
            pltpu.VMEM((sets, model_width, hidden_units), bf16),
            pltpu.VMEM((sets, hidden_units, model_width), bf16),
            pltpu.SemaphoreType.DMA((sets, 2 + down_blocks)),
        ],
        name="expert",
        interpret=INTERPRET,
    )(rows, norm_gain.reshape(2 * y_count, 1, lane), *weight_sets)
    pieces = lax.all_to_all(out_rows, TP, split_axis=0, concat_axis=0, tiled=True)
    expert_out = jnp.sum(
        pieces.reshape(y_count // 2, 4, quarter, local_width).astype(f32), axis=0
    ).astype(bf16)
    back = lax.all_to_all(
        expert_out.reshape(sp_count, capacity, local_width), SP, split_axis=0, concat_axis=0, tiled=True
    ).reshape(slot_total, local_width)
    mixture = jnp.dot(give_first, back, preferred_element_type=f32) + jnp.dot(
        give_rest, back, preferred_element_type=f32
    )
    return (stream.astype(f32) + mixture).astype(bf16)


def solution(mesh):
    sp_count, tp_count = mesh.shape["sp"], mesh.shape["tp"]
    x_count = 4 if sp_count % 8 == 0 else 2
    finer = Mesh(
        mesh.devices.reshape(sp_count // x_count, x_count, tp_count // 2, 2), ("z", "x", "y", "c")
    )
    in_specs = (
        P(SP, TP),
        P(TP, SP),
        P(TP, SP),
        P(TP, SP),
        P(TP, SP),
        P(TP, None),
        P(),
        P(SP, None),
        P(SP, None),
        P(SP, None, TP),
        P(SP, None, TP),
        P(SP, TP, None),
    )
    return jax.shard_map(
        shards, mesh=finer, in_specs=in_specs, out_specs=P(SP, TP), check_vma=False
    )
```

```python
import functools

import jax
import jax.numpy as jnp
from jax import lax
from jax.experimental import pallas as pl
from jax.experimental.pallas import tpu as pltpu
from jax.sharding import Mesh
from jax.sharding import PartitionSpec as P


SP = ("z", "x")
TP = ("y", "c")
INTERPRET = False

norm_eps = 1e-06
masked_score = -1e30
extra_rows = 16
lane = 128


def swapped(shard):
    return lax.ppermute(shard, "c", [(0, 1), (1, 0)])


def three_parts(full):
    parts = []
    for _ in range(3):
        part = full.astype(jnp.bfloat16).astype(jnp.float32)
        full = full - part
        parts.append(part)
    return parts


def pack_kernel(head_width, keys_ref, values_ref, gates_ref, queries_ref, out_ref, query_ref):
    tokens = keys_ref.shape[1]
    head_count = gates_ref.shape[0]
    row = lax.broadcasted_iota(jnp.int32, (extra_rows, tokens), 0)
    gates = jnp.zeros((extra_rows, tokens), jnp.float32)
    for head in range(head_count):
        for place, part in enumerate(three_parts(gates_ref[head : head + 1])):
            gates = jnp.where(row == 3 * head + place, part, gates)
    message = jnp.concatenate(
        [keys_ref[...], values_ref[...], gates.astype(jnp.bfloat16)], axis=0
    )
    for copy in range(out_ref.shape[0]):
        out_ref[copy] = message
    query_ref[...] = queries_ref[...] * jnp.asarray(head_width ** (-0.5), jnp.bfloat16)


def attend_kernel(head_count, head_width, place_ref, kv_ref, *refs):
    out_ref, query_scratch, key_scratch, value_scratch = refs[-4:]
    query_refs = refs[:-4]
    tokens = kv_ref.shape[2]
    z_count, x_count = kv_ref.shape[0], len(query_refs)
    z_place, x_place = place_ref[0], place_ref[1]
    row = lax.broadcasted_iota(jnp.int32, (extra_rows, tokens), 0)
    ones = jnp.ones((extra_rows, tokens), jnp.bfloat16)
    for head in range(head_count):
        minus = jnp.where((row >= 3 * head) & (row < 3 * head + 3), -1.0, 0.0).astype(jnp.bfloat16)
        rows = slice(head * head_width, (head + 1) * head_width)
        for shift in range(x_count):
            target = lax.rem(x_place + x_count - shift, x_count)
            columns = pl.ds(pl.multiple_of(target * tokens, tokens), tokens)
            query_scratch[head, :head_width, columns] = query_refs[shift][rows]
            query_scratch[head, head_width:, columns] = minus
        for block in range(z_count):
            columns = slice(block * tokens, (block + 1) * tokens)
            first = (head_count + head) * head_width
            key_scratch[head, :head_width, columns] = kv_ref[block, rows]
            key_scratch[head, head_width:, columns] = kv_ref[block, 2 * head_count * head_width :]
            value_scratch[head, :head_width, columns] = kv_ref[block, first : first + head_width]
            value_scratch[head, head_width:, columns] = ones
    wide = 2 * tokens if x_count % 2 == 0 else tokens
    stats = [jnp.zeros((extra_rows, tokens), jnp.float32)] * x_count
    for head in range(head_count):
        rows = slice(head * head_width, (head + 1) * head_width)
        for first in range(0, x_count * tokens, wide):
            scores = lax.dot_general(
                key_scratch[head],
                query_scratch[head, :, first : first + wide],
                (((0,), (0,)), ((), ())),
                preferred_element_type=jnp.float32,
            )
            key_row = lax.broadcasted_iota(jnp.int32, scores.shape, 0)
            key_place = key_row // tokens * (x_count * tokens) + key_row % tokens
            key_place = key_place + x_place * tokens
            query_place = lax.broadcasted_iota(jnp.int32, scores.shape, 1)
            query_place = query_place + (z_place * (x_count * tokens) + first)
            scores = jnp.where(key_place <= query_place, scores, 2 * masked_score)
            peak = jnp.maximum(jnp.max(scores, axis=0, keepdims=True), masked_score)
            weights = jnp.exp(scores - peak).astype(jnp.bfloat16)
            summed = jnp.dot(value_scratch[head], weights, preferred_element_type=jnp.float32)
            for block in range(first // tokens, (first + wide) // tokens):
                columns = slice(block * tokens - first, (block + 1) * tokens - first)
                part_sum = summed[:head_width, columns].astype(jnp.bfloat16)
                total = summed[head_width : head_width + 1, columns]
                for place, part in enumerate(three_parts(peak[:, columns]) + three_parts(total)):
                    stats[block] = jnp.where(row == 6 * head + place, part, stats[block])
                for core in range(2):
                    out_ref[block, core, rows] = part_sum
    for block in range(x_count):
        for core in range(2):
            out_ref[block, core, head_count * head_width :] = stats[block].astype(jnp.bfloat16)


def project_kernel(head_count, head_width, place_ref, parts_ref, weight_ref, far_weight_ref, out_ref, weight_scratch):
    x_count = parts_ref.shape[0]
    blocks = out_ref.shape[0]
    width = head_count * head_width
    core = place_ref[2]
    rows = []
    for side, at in ((0, core), (1, 1 - core)):
        source = (weight_ref, far_weight_ref)[side]
        for block in range(blocks):
            columns = pl.ds(pl.multiple_of((block * 2 + core) * lane, lane), lane)
            weight_scratch[side * width : (side + 1) * width, block * lane : (block + 1) * lane] = (
                source[:, columns]
            )
        stats = [parts_ref[part, at, width:].astype(jnp.float32) for part in range(x_count)]
        for head in range(head_count):
            base = 6 * head
            peaks = [
                kept[base : base + 1] + kept[base + 1 : base + 2] + kept[base + 2 : base + 3]
                for kept in stats
            ]
            totals = [
                kept[base + 3 : base + 4] + kept[base + 4 : base + 5] + kept[base + 5 : base + 6]
                for kept in stats
            ]
            top = functools.reduce(jnp.maximum, peaks)
            factors = [jnp.exp(peak - top) for peak in peaks]
            total = sum(factor * amount for factor, amount in zip(factors, totals))
            summed = sum(
                parts_ref[part, at, head * head_width : (head + 1) * head_width].astype(jnp.float32)
                * factors[part]
                for part in range(x_count)
            )
            rows.append((summed / total).astype(jnp.bfloat16))
    attended = jnp.concatenate(rows, axis=0)
    projected = lax.dot_general(
        attended, weight_scratch[...], (((0,), (0,)), ((), ())), preferred_element_type=jnp.float32
    ).astype(jnp.bfloat16)
    for block in range(blocks):
        out_ref[block] = projected[:, block * lane : (block + 1) * lane]


def pack_weights_kernel(gate_ref, up_ref, down_ref, out_ref, held, in_sems, out_sems):
    units = gate_ref.shape[1]
    groups = [
        [pltpu.make_async_copy(gate_ref, held.at[0], in_sems.at[0])],
        [pltpu.make_async_copy(up_ref, held.at[1], in_sems.at[1])],
        [],
    ]
    for block in range(down_ref.shape[1] // units):
        columns = pl.ds(block * units, units)
        groups[2].append(
            pltpu.make_async_copy(
                down_ref.at[:, columns], held.at[2, columns, :], in_sems.at[2 + block]
            )
        )
    for group in groups:
        for copy in group:
            copy.start()
    outward = []
    for kind, group in enumerate(groups):
        for copy in group:
            copy.wait()
        outward.append(pltpu.make_async_copy(held.at[kind], out_ref.at[kind], out_sems.at[kind]))
        outward[kind].start()
    for copy in outward:
        copy.wait()


def expert_kernel(rows_in_ref, gain_ref, *refs):
    sets = len(refs) - 8
    set_refs = refs[:sets]
    out_ref, rows_ref, hidden_ref, full_ref, gates, ups, downs, sems = refs[sets:]
    blocks = rows_in_ref.shape[0]
    width = rows_ref.shape[1]
    units = gates.shape[2]
    gate_copies, up_copies, down_copies = [], [], []
    for part in range(sets):
        gate_copies.append(
            pltpu.make_async_copy(set_refs[part].at[0], gates.at[part], sems.at[part, 0])
        )
        up_copies.append(pltpu.make_async_copy(set_refs[part].at[1], ups.at[part], sems.at[part, 1]))
        gate_copies[part].start()
        up_copies[part].start()
    for part in range(sets):
        for block in range(width // units):
            columns = pl.ds(block * units, units)
            down_copies.append(
                pltpu.make_async_copy(
                    set_refs[part].at[2, columns, :], downs.at[part, :, columns], sems.at[part, 2 + block]
                )
            )
            down_copies[-1].start()
    squares = jnp.zeros(rows_in_ref.shape[1:], jnp.float32)
    for block in range(blocks):
        values = rows_in_ref[block].astype(jnp.float32)
        squares = squares + values * values
    scale = lax.rsqrt(jnp.sum(squares, axis=1, keepdims=True) / width + norm_eps)
    for block in range(blocks):
        values = rows_in_ref[block].astype(jnp.float32) * scale * gain_ref[block]
        rows_ref[:, block * lane : (block + 1) * lane] = values.astype(jnp.bfloat16)
    for part in range(sets):
        gate_copies[part].wait()
        gate = jnp.dot(rows_ref[...], gates[part], preferred_element_type=jnp.float32)
        up_copies[part].wait()
        up = jnp.dot(rows_ref[...], ups[part], preferred_element_type=jnp.float32)
        hidden_ref[:, part * units : (part + 1) * units] = (
            gate / (1.0 + jnp.exp(-gate)) * up
        ).astype(jnp.bfloat16)
    for copy in down_copies:
        copy.wait()
    full_ref[...] = jnp.dot(
        hidden_ref[...], downs[...].reshape(sets * units, width), preferred_element_type=jnp.float32
    ).astype(jnp.bfloat16)
    for block in range(blocks):
        out_ref[block] = full_ref[:, block * lane : (block + 1) * lane]


def shards(
    residual,
    queries,
    keys,
    values,
    forget_cache,
    out_weight,
    norm_gain,
    routes,
    route_weight,
    gate_weight,
    up_weight,
    down_weight,
):
    z_count, x_count, y_count = (lax.axis_size(axis) for axis in ("z", "x", "y"))
    sp_count = z_count * x_count
    token_count, local_width = residual.shape
    model_width = norm_gain.shape[0]
    head_count = forget_cache.shape[0]
    head_width = queries.shape[0] // head_count
    top_count = routes.shape[1]
    capacity = max(2, token_count * top_count * 5 // (4 * sp_count))
    slot_total = sp_count * capacity
    bf16, f32 = jnp.bfloat16, jnp.float32
    place = jnp.stack(
        [lax.axis_index("z"), lax.axis_index("x"), lax.axis_index("c"), lax.axis_index("y")]
    ).astype(jnp.int32)
    smem = pl.BlockSpec(memory_space=pltpu.SMEM)
    vmem = pl.BlockSpec(memory_space=pltpu.VMEM)

    deep = head_width + extra_rows
    message_rows = 2 * head_count * head_width + extra_rows
    message, scaled = pl.pallas_call(
        functools.partial(pack_kernel, head_width),
        out_shape=(
            jax.ShapeDtypeStruct((z_count, message_rows, token_count), bf16),
            jax.ShapeDtypeStruct(queries.shape, bf16),
        ),
        in_specs=[vmem] * 4,
        out_specs=(vmem, vmem),
        name="pack",
        interpret=INTERPRET,
    )(keys, values, forget_cache, queries)
    gathered = lax.all_to_all(message, "z", split_axis=0, concat_axis=0, tiled=True)
    query_list = [scaled] + [
        lax.ppermute(scaled, "x", [(i, (i + shift) % x_count) for i in range(x_count)])
        for shift in range(1, x_count)
    ]
    slice_moves = []
    for y_from in range(y_count):
        slice_moves.append((2 * y_from, 2 * ((y_from - 1) % y_count)))
        slice_moves.append((2 * y_from + 1, 2 * ((y_from + 1) % y_count) + 1))
    hidden_units = gate_weight.shape[2]
    any_space = pl.BlockSpec(memory_space=pl.ANY)
    down_blocks = model_width // hidden_units
    own_set = pl.pallas_call(
        pack_weights_kernel,
        out_shape=jax.ShapeDtypeStruct((3, model_width, hidden_units), bf16),
        in_specs=[any_space] * 3,
        out_specs=any_space,
        scratch_shapes=[
            pltpu.VMEM((3, model_width, hidden_units), bf16),
            pltpu.SemaphoreType.DMA((2 + down_blocks,)),
            pltpu.SemaphoreType.DMA((3,)),
        ],
        name="pack_weights",
        interpret=INTERPRET,
    )(gate_weight[0], up_weight[0], down_weight[0])
    near_set = lax.ppermute(own_set, TP, slice_moves)
    own_swapped = swapped(own_set)
    far_out_weight = swapped(out_weight)
    near_swapped = swapped(near_set)
    attend = pl.pallas_call(
        functools.partial(attend_kernel, head_count, head_width),
        out_shape=jax.ShapeDtypeStruct(
            (x_count, 2, head_count * head_width + extra_rows, token_count), bf16
        ),
        in_specs=[smem] + [vmem] * (1 + x_count),
        out_specs=vmem,
        scratch_shapes=[
            pltpu.VMEM((head_count, deep, x_count * token_count), bf16),
            pltpu.VMEM((head_count, deep, z_count * token_count), bf16),
            pltpu.VMEM((head_count, deep, z_count * token_count), bf16),
        ],
        name="attend",
        interpret=INTERPRET,
    )
    parts = attend(place, gathered, *query_list)
    part_shape = parts.shape
    received = lax.all_to_all(
        parts.reshape(2 * x_count, *part_shape[2:]), ("x", "c"), split_axis=0, concat_axis=0, tiled=True
    ).reshape(part_shape)

    expert_ids = jnp.arange(sp_count, dtype=jnp.int32)
    chosen = routes[:, :, None] == expert_ids
    named = jnp.any(chosen, axis=1)
    token_ids = jnp.arange(token_count, dtype=jnp.int32)
    before = (token_ids[None, :] < token_ids[:, None]).astype(bf16)
    rank = jnp.dot(before, named.astype(bf16), preferred_element_type=f32).astype(jnp.int32)
    slot_ids = jnp.arange(capacity, dtype=jnp.int32)
    taken = (named.T[:, None, :] & (rank.T[:, None, :] == slot_ids[:, None])).astype(bf16)
    taken = taken.reshape(slot_total, token_count)
    share = jnp.sum(jnp.where(chosen, route_weight[:, :, None], 0.0), axis=1)
    share_first = lax.reduce_precision(share, 8, 7)
    share_rest = (share - share_first).astype(bf16)

    def spread(weights):
        return jnp.where(
            rank[:, :, None] == slot_ids, weights.astype(bf16)[:, :, None], jnp.zeros((), bf16)
        ).reshape(token_count, slot_total)

    give_first, give_rest = spread(share_first), spread(share_rest)

    projected = pl.pallas_call(
        functools.partial(project_kernel, head_count, head_width),
        out_shape=jax.ShapeDtypeStruct((y_count, token_count, local_width), bf16),
        in_specs=[smem, vmem, vmem, vmem],
        out_specs=vmem,
        scratch_shapes=[pltpu.VMEM((2 * head_count * head_width, y_count * local_width), bf16)],
        name="project",
        interpret=INTERPRET,
    )(place, received, out_weight, far_out_weight)
    pieces = lax.all_to_all(projected, "y", split_axis=0, concat_axis=0, tiled=True)
    pieces, own_swapped, near_set, near_swapped = lax.optimization_barrier(
        (pieces, own_swapped, near_set, near_swapped)
    )
    weight_sets = [own_set, own_swapped, near_set, near_swapped]
    head_sum = jnp.sum(pieces.astype(f32), axis=0)
    stream = (residual.astype(f32) + head_sum).astype(bf16)

    sent = jnp.dot(taken, stream, preferred_element_type=f32).astype(bf16)
    arrived = lax.all_to_all(
        sent.reshape(sp_count, capacity, local_width), SP, split_axis=0, concat_axis=0, tiled=True
    )
    quarter = slot_total // 4
    arrived = arrived.reshape(4, quarter, local_width)
    copies = jnp.broadcast_to(arrived, (y_count // 2, *arrived.shape))
    rows = lax.all_to_all(
        copies.reshape(2 * y_count, quarter, local_width), TP, split_axis=0, concat_axis=0, tiled=True
    )
    sets = len(weight_sets)
    out_rows = pl.pallas_call(
        expert_kernel,
        out_shape=jax.ShapeDtypeStruct((2 * y_count, quarter, local_width), bf16),
        in_specs=[vmem, vmem] + [any_space] * sets,
        out_specs=vmem,
        scratch_shapes=[
            pltpu.VMEM((quarter, model_width), bf16),
            pltpu.VMEM((quarter, sets * hidden_units), bf16),
            pltpu.VMEM((quarter, model_width), bf16),
            pltpu.VMEM((sets, model_width, hidden_units), bf16),
            pltpu.VMEM((sets, model_width, hidden_units), bf16),
            pltpu.VMEM((sets, hidden_units, model_width), bf16),
            pltpu.SemaphoreType.DMA((sets, 2 + down_blocks)),
        ],
        name="expert",
        interpret=INTERPRET,
    )(rows, norm_gain.reshape(2 * y_count, 1, lane), *weight_sets)
    pieces = lax.all_to_all(out_rows, TP, split_axis=0, concat_axis=0, tiled=True)
    expert_out = jnp.sum(
        pieces.reshape(y_count // 2, 4, quarter, local_width).astype(f32), axis=0
    ).astype(bf16)
    back = lax.all_to_all(
        expert_out.reshape(sp_count, capacity, local_width), SP, split_axis=0, concat_axis=0, tiled=True
    ).reshape(slot_total, local_width)
    mixture = jnp.dot(give_first, back, preferred_element_type=f32) + jnp.dot(
        give_rest, back, preferred_element_type=f32
    )
    return (stream.astype(f32) + mixture).astype(bf16)


def solution(mesh):
    sp_count, tp_count = mesh.shape["sp"], mesh.shape["tp"]
    x_count = 4 if sp_count % 8 == 0 else 2
    finer = Mesh(
        mesh.devices.reshape(sp_count // x_count, x_count, tp_count // 2, 2), ("z", "x", "y", "c")
    )
    in_specs = (
        P(SP, TP),
        P(TP, SP),
        P(TP, SP),
        P(TP, SP),
        P(TP, SP),
        P(TP, None),
        P(),
        P(SP, None),
        P(SP, None),
        P(SP, None, TP),
        P(SP, None, TP),
        P(SP, TP, None),
    )
    return jax.shard_map(
        shards, mesh=finer, in_specs=in_specs, out_specs=P(SP, TP), check_vma=False
    )
```

```python
import functools

import jax
import jax.numpy as jnp
from jax import lax
from jax.experimental import pallas as pl
from jax.experimental.pallas import tpu as pltpu
from jax.sharding import Mesh
from jax.sharding import PartitionSpec as P


SP = ("z", "x")
TP = ("y", "c")
INTERPRET = False

norm_eps = 1e-06
masked_score = -1e30
extra_rows = 16
lane = 128


def held(array):
    return array if INTERPRET else pltpu.with_memory_space_constraint(array, pltpu.VMEM)


def kept(shape, dtype):
    return jax.ShapeDtypeStruct(shape, dtype) if INTERPRET else pltpu.VMEM(shape, dtype)


def swapped(shard):
    return lax.ppermute(shard, "c", [(0, 1), (1, 0)])


def three_parts(full):
    parts = []
    for _ in range(3):
        part = full.astype(jnp.bfloat16).astype(jnp.float32)
        full = full - part
        parts.append(part)
    return parts


def pack_kernel(head_width, keys_ref, values_ref, gates_ref, queries_ref, out_ref, query_ref):
    tokens = keys_ref.shape[1]
    head_count = gates_ref.shape[0]
    row = lax.broadcasted_iota(jnp.int32, (extra_rows, tokens), 0)
    gates = jnp.zeros((extra_rows, tokens), jnp.float32)
    for head in range(head_count):
        for place, part in enumerate(three_parts(gates_ref[head : head + 1])):
            gates = jnp.where(row == 3 * head + place, part, gates)
    message = jnp.concatenate(
        [keys_ref[...], values_ref[...], gates.astype(jnp.bfloat16)], axis=0
    )
    for copy in range(out_ref.shape[0]):
        out_ref[copy] = message
    query_ref[...] = queries_ref[...] * jnp.asarray(head_width ** (-0.5), jnp.bfloat16)


def attend_kernel(head_count, head_width, place_ref, kv_ref, *refs):
    out_ref, query_scratch, key_scratch, value_scratch = refs[-4:]
    query_refs = refs[:-4]
    tokens = kv_ref.shape[2]
    z_count, x_count = kv_ref.shape[0], len(query_refs)
    z_place, x_place = place_ref[0], place_ref[1]
    row = lax.broadcasted_iota(jnp.int32, (extra_rows, tokens), 0)
    ones = jnp.ones((extra_rows, tokens), jnp.bfloat16)
    for head in range(head_count):
        counted = ((row >= 3 * head) & (row < 3 * head + 3)) | (row == extra_rows - 1)
        minus = jnp.where(counted, -1.0, 0.0).astype(jnp.bfloat16)
        rows = slice(head * head_width, (head + 1) * head_width)
        for shift in range(x_count):
            target = lax.rem(x_place + x_count - shift, x_count)
            columns = pl.ds(pl.multiple_of(target * tokens, tokens), tokens)
            query_scratch[head, :head_width, columns] = query_refs[shift][rows]
            query_scratch[head, head_width:, columns] = minus
        for block in range(z_count):
            source = lax.rem(z_place + block, z_count)
            columns = slice(block * tokens, (block + 1) * tokens)
            first = (head_count + head) * head_width
            later = jnp.where((block > 0) & (z_place + block < z_count), -2 * masked_score, 0.0)
            gates = kv_ref[source, 2 * head_count * head_width :]
            key_scratch[head, :head_width, columns] = kv_ref[source, rows]
            key_scratch[head, head_width:, columns] = jnp.where(
                row == extra_rows - 1, later, gates.astype(jnp.float32)
            ).astype(jnp.bfloat16)
            value_scratch[head, :head_width, columns] = kv_ref[source, first : first + head_width]
            value_scratch[head, head_width:, columns] = ones
    wide = 2 * tokens if x_count % 2 == 0 else tokens
    stats = [jnp.zeros((extra_rows, tokens), jnp.float32)] * x_count
    for head in range(head_count):
        rows = slice(head * head_width, (head + 1) * head_width)
        for first in range(0, x_count * tokens, wide):
            scores = lax.dot_general(
                key_scratch[head],
                query_scratch[head, :, first : first + wide],
                (((0,), (0,)), ((), ())),
                preferred_element_type=jnp.float32,
            )
            near = scores[:tokens]
            key_place = lax.broadcasted_iota(jnp.int32, near.shape, 0) + x_place * tokens
            query_place = lax.broadcasted_iota(jnp.int32, near.shape, 1) + first
            near = jnp.where(key_place <= query_place, near, 2 * masked_score)
            scores = jnp.concatenate([near, scores[tokens:]], axis=0)
            peak = jnp.maximum(jnp.max(scores, axis=0, keepdims=True), masked_score)
            weights = jnp.exp(scores - peak).astype(jnp.bfloat16)
            summed = jnp.dot(value_scratch[head], weights, preferred_element_type=jnp.float32)
            for block in range(first // tokens, (first + wide) // tokens):
                columns = slice(block * tokens - first, (block + 1) * tokens - first)
                part_sum = summed[:head_width, columns].astype(jnp.bfloat16)
                total = summed[head_width : head_width + 1, columns]
                for place, part in enumerate(three_parts(peak[:, columns]) + three_parts(total)):
                    stats[block] = jnp.where(row == 6 * head + place, part, stats[block])
                for core in range(2):
                    out_ref[block, core, rows] = part_sum
    for block in range(x_count):
        for core in range(2):
            out_ref[block, core, head_count * head_width :] = stats[block].astype(jnp.bfloat16)


def project_kernel(head_count, head_width, place_ref, parts_ref, weight_ref, far_weight_ref, out_ref, weight_scratch):
    x_count = parts_ref.shape[0]
    blocks = out_ref.shape[0]
    width = head_count * head_width
    core = place_ref[2]
    rows = []
    for side, at in ((0, core), (1, 1 - core)):
        source = (weight_ref, far_weight_ref)[side]
        for block in range(blocks):
            columns = pl.ds(pl.multiple_of((block * 2 + core) * lane, lane), lane)
            weight_scratch[side * width : (side + 1) * width, block * lane : (block + 1) * lane] = (
                source[:, columns]
            )
        stats = [parts_ref[part, at, width:].astype(jnp.float32) for part in range(x_count)]
        for head in range(head_count):
            base = 6 * head
            peaks = [
                kept[base : base + 1] + kept[base + 1 : base + 2] + kept[base + 2 : base + 3]
                for kept in stats
            ]
            totals = [
                kept[base + 3 : base + 4] + kept[base + 4 : base + 5] + kept[base + 5 : base + 6]
                for kept in stats
            ]
            top = functools.reduce(jnp.maximum, peaks)
            factors = [jnp.exp(peak - top) for peak in peaks]
            total = sum(factor * amount for factor, amount in zip(factors, totals))
            summed = sum(
                parts_ref[part, at, head * head_width : (head + 1) * head_width].astype(jnp.float32)
                * factors[part]
                for part in range(x_count)
            )
            rows.append((summed / total).astype(jnp.bfloat16))
    attended = jnp.concatenate(rows, axis=0)
    projected = lax.dot_general(
        attended, weight_scratch[...], (((0,), (0,)), ((), ())), preferred_element_type=jnp.float32
    ).astype(jnp.bfloat16)
    for block in range(blocks):
        out_ref[block] = projected[:, block * lane : (block + 1) * lane]


def pack_weights_kernel(gate_ref, up_ref, down_ref, out_ref, held, in_sems, out_sems):
    units = gate_ref.shape[1]
    groups = [
        [pltpu.make_async_copy(gate_ref, held.at[0], in_sems.at[0])],
        [pltpu.make_async_copy(up_ref, held.at[1], in_sems.at[1])],
        [],
    ]
    for block in range(down_ref.shape[1] // units):
        columns = pl.ds(block * units, units)
        groups[2].append(
            pltpu.make_async_copy(
                down_ref.at[:, columns], held.at[2, columns, :], in_sems.at[2 + block]
            )
        )
    for group in groups:
        for copy in group:
            copy.start()
    outward = []
    for kind, group in enumerate(groups):
        for copy in group:
            copy.wait()
        outward.append(pltpu.make_async_copy(held.at[kind], out_ref.at[kind], out_sems.at[kind]))
        outward[kind].start()
    for copy in outward:
        copy.wait()


def expert_kernel(rows_in_ref, gain_ref, *refs):
    sets = len(refs) - 5
    out_ref, rows_ref, hidden_ref, kinds, sems = refs[sets:]
    blocks = rows_in_ref.shape[0]
    width = rows_ref.shape[1]
    units = kinds.shape[3]
    copies = [
        [pltpu.make_async_copy(refs[part].at[kind], kinds.at[part, kind], sems.at[part, kind]) for kind in range(3)]
        for part in range(sets)
    ]
    for part in range(sets):
        copies[part][0].start()
        copies[part][1].start()
    for part in range(sets):
        copies[part][2].start()
    squares = jnp.zeros(rows_in_ref.shape[1:], jnp.float32)
    for block in range(blocks):
        values = rows_in_ref[block].astype(jnp.float32)
        squares = squares + values * values
    scale = lax.rsqrt(jnp.sum(squares, axis=1, keepdims=True) / width + norm_eps)
    for block in range(blocks):
        values = rows_in_ref[block].astype(jnp.float32) * scale * gain_ref[block]
        rows_ref[:, block * lane : (block + 1) * lane] = values.astype(jnp.bfloat16)
    for part in range(sets):
        copies[part][0].wait()
        gate = jnp.dot(rows_ref[...], kinds[part, 0], preferred_element_type=jnp.float32)
        copies[part][1].wait()
        up = jnp.dot(rows_ref[...], kinds[part, 1], preferred_element_type=jnp.float32)
        hidden_ref[part] = (gate / (1.0 + jnp.exp(-gate)) * up).astype(jnp.bfloat16)
    for part in range(sets):
        copies[part][2].wait()
    for block in range(width // units):
        down_rows = slice(block * units, (block + 1) * units)
        total = sum(
            jnp.dot(hidden_ref[part], kinds[part, 2, down_rows, :], preferred_element_type=jnp.float32)
            for part in range(sets)
        ).astype(jnp.bfloat16)
        for piece in range(units // lane):
            out_ref[block * (units // lane) + piece] = total[:, piece * lane : (piece + 1) * lane]


def shards(
    residual,
    queries,
    keys,
    values,
    forget_cache,
    out_weight,
    norm_gain,
    routes,
    route_weight,
    gate_weight,
    up_weight,
    down_weight,
):
    z_count, x_count, y_count = (lax.axis_size(axis) for axis in ("z", "x", "y"))
    sp_count = z_count * x_count
    token_count, local_width = residual.shape
    model_width = norm_gain.shape[0]
    head_count = forget_cache.shape[0]
    head_width = queries.shape[0] // head_count
    top_count = routes.shape[1]
    capacity = max(2, token_count * top_count * 5 // (4 * sp_count))
    slot_total = sp_count * capacity
    bf16, f32 = jnp.bfloat16, jnp.float32
    place = jnp.stack(
        [lax.axis_index("z"), lax.axis_index("x"), lax.axis_index("c"), lax.axis_index("y")]
    ).astype(jnp.int32)
    smem = pl.BlockSpec(memory_space=pltpu.SMEM)
    vmem = pl.BlockSpec(memory_space=pltpu.VMEM)

    deep = head_width + extra_rows
    message_rows = 2 * head_count * head_width + extra_rows
    message, scaled = pl.pallas_call(
        functools.partial(pack_kernel, head_width),
        out_shape=(
            jax.ShapeDtypeStruct((z_count, message_rows, token_count), bf16),
            kept(queries.shape, bf16),
        ),
        in_specs=[vmem] * 4,
        out_specs=(vmem, vmem),
        name="pack",
        interpret=INTERPRET,
    )(keys, values, forget_cache, queries)
    gathered = lax.all_to_all(message, "z", split_axis=0, concat_axis=0, tiled=True)
    query_list = [scaled] + [
        lax.ppermute(scaled, "x", [(i, (i + shift) % x_count) for i in range(x_count)])
        for shift in range(1, x_count)
    ]
    slice_moves = []
    for y_from in range(y_count):
        slice_moves.append((2 * y_from, 2 * ((y_from - 1) % y_count)))
        slice_moves.append((2 * y_from + 1, 2 * ((y_from + 1) % y_count) + 1))
    hidden_units = gate_weight.shape[2]
    any_space = pl.BlockSpec(memory_space=pl.ANY)
    down_blocks = model_width // hidden_units
    own_set = pl.pallas_call(
        pack_weights_kernel,
        out_shape=jax.ShapeDtypeStruct((3, model_width, hidden_units), bf16),
        in_specs=[any_space] * 3,
        out_specs=any_space,
        scratch_shapes=[
            pltpu.VMEM((3, model_width, hidden_units), bf16),
            pltpu.SemaphoreType.DMA((2 + down_blocks,)),
            pltpu.SemaphoreType.DMA((3,)),
        ],
        name="pack_weights",
        interpret=INTERPRET,
    )(gate_weight[0], up_weight[0], down_weight[0])
    near_set = lax.ppermute(own_set, TP, slice_moves)
    own_swapped = swapped(own_set)
    far_out_weight = swapped(out_weight)
    near_swapped = swapped(near_set)
    attend = pl.pallas_call(
        functools.partial(attend_kernel, head_count, head_width),
        out_shape=jax.ShapeDtypeStruct(
            (x_count, 2, head_count * head_width + extra_rows, token_count), bf16
        ),
        in_specs=[smem] + [vmem] * (1 + x_count),
        out_specs=vmem,
        scratch_shapes=[
            pltpu.VMEM((head_count, deep, x_count * token_count), bf16),
            pltpu.VMEM((head_count, deep, z_count * token_count), bf16),
            pltpu.VMEM((head_count, deep, z_count * token_count), bf16),
        ],
        name="attend",
        interpret=INTERPRET,
    )
    parts = attend(place, held(gathered), *map(held, query_list))
    part_shape = parts.shape
    received = lax.all_to_all(
        parts.reshape(2 * x_count, *part_shape[2:]), ("x", "c"), split_axis=0, concat_axis=0, tiled=True
    ).reshape(part_shape)

    expert_ids = jnp.arange(sp_count, dtype=jnp.int32)
    chosen = routes[:, :, None] == expert_ids
    named = jnp.any(chosen, axis=1)
    token_ids = jnp.arange(token_count, dtype=jnp.int32)
    before = (token_ids[None, :] < token_ids[:, None]).astype(bf16)
    rank = jnp.dot(before, named.astype(bf16), preferred_element_type=f32).astype(jnp.int32)
    slot_ids = jnp.arange(capacity, dtype=jnp.int32)
    taken = (named.T[:, None, :] & (rank.T[:, None, :] == slot_ids[:, None])).astype(bf16)
    taken = taken.reshape(slot_total, token_count)
    share = jnp.sum(jnp.where(chosen, route_weight[:, :, None], 0.0), axis=1)
    share_first = lax.reduce_precision(share, 8, 7)
    share_rest = (share - share_first).astype(bf16)

    def spread(weights):
        return jnp.where(
            rank[:, :, None] == slot_ids, weights.astype(bf16)[:, :, None], jnp.zeros((), bf16)
        ).reshape(token_count, slot_total)

    give_first, give_rest = spread(share_first), spread(share_rest)

    projected = pl.pallas_call(
        functools.partial(project_kernel, head_count, head_width),
        out_shape=jax.ShapeDtypeStruct((y_count, token_count, local_width), bf16),
        in_specs=[smem, vmem, vmem, vmem],
        out_specs=vmem,
        scratch_shapes=[pltpu.VMEM((2 * head_count * head_width, y_count * local_width), bf16)],
        name="project",
        interpret=INTERPRET,
    )(place, held(received), held(out_weight), held(far_out_weight))
    pieces = lax.all_to_all(projected, "y", split_axis=0, concat_axis=0, tiled=True)
    pieces, own_swapped, near_set, near_swapped = lax.optimization_barrier(
        (pieces, own_swapped, near_set, near_swapped)
    )
    weight_sets = [own_set, own_swapped, near_set, near_swapped]
    head_sum = jnp.sum(pieces.astype(f32), axis=0)
    stream = (residual.astype(f32) + head_sum).astype(bf16)

    sent = jnp.dot(taken, stream, preferred_element_type=f32).astype(bf16)
    arrived = lax.all_to_all(
        sent.reshape(sp_count, capacity, local_width), SP, split_axis=0, concat_axis=0, tiled=True
    )
    quarter = slot_total // 4
    arrived = arrived.reshape(4, quarter, local_width)
    copies = jnp.broadcast_to(arrived, (y_count // 2, *arrived.shape))
    rows = lax.all_to_all(
        copies.reshape(2 * y_count, quarter, local_width), TP, split_axis=0, concat_axis=0, tiled=True
    )
    sets = len(weight_sets)
    out_rows = pl.pallas_call(
        expert_kernel,
        out_shape=kept((2 * y_count, quarter, local_width), bf16),
        in_specs=[vmem, vmem] + [any_space] * sets,
        out_specs=vmem,
        scratch_shapes=[
            pltpu.VMEM((quarter, model_width), bf16),
            pltpu.VMEM((sets, quarter, hidden_units), bf16),
            pltpu.VMEM((sets, 3, model_width, hidden_units), bf16),
            pltpu.SemaphoreType.DMA((sets, 3)),
        ],
        name="expert",
        interpret=INTERPRET,
    )(held(rows), norm_gain.reshape(2 * y_count, 1, lane), *weight_sets)
    pieces = lax.all_to_all(out_rows, TP, split_axis=0, concat_axis=0, tiled=True)
    expert_out = jnp.sum(
        pieces.reshape(y_count // 2, 4, quarter, local_width).astype(f32), axis=0
    ).astype(bf16)
    back = lax.all_to_all(
        expert_out.reshape(sp_count, capacity, local_width), SP, split_axis=0, concat_axis=0, tiled=True
    ).reshape(slot_total, local_width)
    mixture = jnp.dot(give_first, back, preferred_element_type=f32) + jnp.dot(
        give_rest, back, preferred_element_type=f32
    )
    return (stream.astype(f32) + mixture).astype(bf16)


def solution(mesh):
    sp_count, tp_count = mesh.shape["sp"], mesh.shape["tp"]
    x_count = 4 if sp_count % 8 == 0 else 2
    finer = Mesh(
        mesh.devices.reshape(sp_count // x_count, x_count, tp_count // 2, 2), ("z", "x", "y", "c")
    )
    in_specs = (
        P(SP, TP),
        P(TP, SP),
        P(TP, SP),
        P(TP, SP),
        P(TP, SP),
        P(TP, None),
        P(),
        P(SP, None),
        P(SP, None),
        P(SP, None, TP),
        P(SP, None, TP),
        P(SP, TP, None),
    )
    return jax.shard_map(
        shards, mesh=finer, in_specs=in_specs, out_specs=P(SP, TP), check_vma=False
    )
```

```python
import functools

import jax
import jax.numpy as jnp
from jax import lax
from jax.experimental import pallas as pl
from jax.experimental.pallas import tpu as pltpu
from jax.sharding import Mesh
from jax.sharding import PartitionSpec as P


SP = ("z", "x")
TP = ("y", "c")
INTERPRET = False

norm_eps = 1e-06
masked_score = -1e30
extra_rows = 16
gate_rows = 8
lane = 128


def held(array):
    return array if INTERPRET else pltpu.with_memory_space_constraint(array, pltpu.VMEM)


def kept(shape, dtype):
    return jax.ShapeDtypeStruct(shape, dtype) if INTERPRET else pltpu.VMEM(shape, dtype)


def swapped(shard):
    return lax.ppermute(shard, "c", [(0, 1), (1, 0)])


def three_parts(full):
    parts = []
    for _ in range(3):
        part = full.astype(jnp.bfloat16).astype(jnp.float32)
        full = full - part
        parts.append(part)
    return parts


def pack_kernel(head_width, keys_ref, values_ref, gates_ref, queries_ref, out_ref, query_ref):
    tokens = keys_ref.shape[1]
    head_count = gates_ref.shape[0]
    row = lax.broadcasted_iota(jnp.int32, (extra_rows, tokens), 0)
    gates = jnp.zeros((extra_rows, tokens), jnp.float32)
    for head in range(head_count):
        for place, part in enumerate(three_parts(gates_ref[head : head + 1])):
            gates = jnp.where(row == 3 * head + place, part, gates)
    message = jnp.concatenate(
        [keys_ref[...], values_ref[...], gates[:gate_rows].astype(jnp.bfloat16)], axis=0
    )
    for copy in range(out_ref.shape[0]):
        out_ref[copy] = message
    query_ref[...] = queries_ref[...] * jnp.asarray(head_width ** (-0.5), jnp.bfloat16)


def attend_kernel(head_count, head_width, place_ref, kv_ref, *refs):
    out_ref, query_scratch, key_scratch, value_scratch = refs[-4:]
    query_refs = refs[:-4]
    tokens = kv_ref.shape[2]
    z_count, x_count = kv_ref.shape[0], len(query_refs)
    z_place, x_place = place_ref[0], place_ref[1]
    row = lax.broadcasted_iota(jnp.int32, (extra_rows, tokens), 0)
    ones = jnp.ones((extra_rows, tokens), jnp.bfloat16)
    for head in range(head_count):
        counted = ((row >= 3 * head) & (row < 3 * head + 3)) | (row == gate_rows - 1)
        minus = jnp.where(counted, -1.0, 0.0).astype(jnp.bfloat16)
        rows = slice(head * head_width, (head + 1) * head_width)
        for shift in range(x_count):
            target = lax.rem(x_place + x_count - shift, x_count)
            columns = pl.ds(pl.multiple_of(target * tokens, tokens), tokens)
            query_scratch[head, :head_width, columns] = query_refs[shift][rows]
            query_scratch[head, head_width:, columns] = minus
        for block in range(z_count):
            source = lax.rem(z_place + block, z_count)
            columns = slice(block * tokens, (block + 1) * tokens)
            first = (head_count + head) * head_width
            later = jnp.where((block > 0) & (z_place + block < z_count), -2 * masked_score, 0.0)
            gates = kv_ref[source, 2 * head_count * head_width :]
            key_scratch[head, :head_width, columns] = kv_ref[source, rows]
            gates = jnp.where(row[:gate_rows] == gate_rows - 1, later, gates.astype(jnp.float32))
            gates = jnp.concatenate([gates, jnp.zeros_like(gates)], axis=0)
            key_scratch[head, head_width:, columns] = gates.astype(jnp.bfloat16)
            value_scratch[head, :head_width, columns] = kv_ref[source, first : first + head_width]
            value_scratch[head, head_width:, columns] = ones
    wide = x_count * tokens
    stats = [jnp.zeros((extra_rows, tokens), jnp.float32)] * x_count
    for head in range(head_count):
        rows = slice(head * head_width, (head + 1) * head_width)
        for first in range(0, x_count * tokens, wide):
            scores = lax.dot_general(
                key_scratch[head],
                query_scratch[head, :, first : first + wide],
                (((0,), (0,)), ((), ())),
                preferred_element_type=jnp.float32,
            )
            near = scores[:tokens]
            key_place = lax.broadcasted_iota(jnp.int32, near.shape, 0) + x_place * tokens
            query_place = lax.broadcasted_iota(jnp.int32, near.shape, 1) + first
            near = jnp.where(key_place <= query_place, near, 2 * masked_score)
            rest = scores[tokens:]
            peak = jnp.maximum(jnp.max(near, axis=0, keepdims=True), jnp.max(rest, axis=0, keepdims=True))
            peak = jnp.maximum(peak, masked_score)
            near_weights = jnp.exp(near - peak).astype(jnp.bfloat16)
            rest_weights = jnp.exp(rest - peak).astype(jnp.bfloat16)
            summed = jnp.dot(
                value_scratch[head, :, :tokens], near_weights, preferred_element_type=jnp.float32
            ) + jnp.dot(value_scratch[head, :, tokens:], rest_weights, preferred_element_type=jnp.float32)
            for block in range(first // tokens, (first + wide) // tokens):
                columns = slice(block * tokens - first, (block + 1) * tokens - first)
                part_sum = summed[:head_width, columns].astype(jnp.bfloat16)
                total = summed[head_width : head_width + 1, columns]
                for place, part in enumerate(three_parts(peak[:, columns]) + three_parts(total)):
                    stats[block] = jnp.where(row == 6 * head + place, part, stats[block])
                for core in range(2):
                    out_ref[block, core, rows] = part_sum
    for block in range(x_count):
        for core in range(2):
            out_ref[block, core, head_count * head_width :] = stats[block].astype(jnp.bfloat16)


def project_kernel(head_count, head_width, place_ref, parts_ref, weight_ref, far_weight_ref, out_ref, weight_scratch):
    x_count = parts_ref.shape[0]
    blocks = out_ref.shape[0]
    width = head_count * head_width
    core = place_ref[2]
    rows = []
    for side, at in ((0, core), (1, 1 - core)):
        source = (weight_ref, far_weight_ref)[side]
        for block in range(blocks):
            columns = pl.ds(pl.multiple_of((block * 2 + core) * lane, lane), lane)
            weight_scratch[side * width : (side + 1) * width, block * lane : (block + 1) * lane] = (
                source[:, columns]
            )
        stats = [parts_ref[part, at, width:].astype(jnp.float32) for part in range(x_count)]
        for head in range(head_count):
            base = 6 * head
            peaks = [
                kept[base : base + 1] + kept[base + 1 : base + 2] + kept[base + 2 : base + 3]
                for kept in stats
            ]
            totals = [
                kept[base + 3 : base + 4] + kept[base + 4 : base + 5] + kept[base + 5 : base + 6]
                for kept in stats
            ]
            top = functools.reduce(jnp.maximum, peaks)
            factors = [jnp.exp(peak - top) for peak in peaks]
            total = sum(factor * amount for factor, amount in zip(factors, totals))
            summed = sum(
                parts_ref[part, at, head * head_width : (head + 1) * head_width].astype(jnp.float32)
                * factors[part]
                for part in range(x_count)
            )
            rows.append((summed / total).astype(jnp.bfloat16))
    attended = jnp.concatenate(rows, axis=0)
    projected = lax.dot_general(
        attended, weight_scratch[...], (((0,), (0,)), ((), ())), preferred_element_type=jnp.float32
    ).astype(jnp.bfloat16)
    for block in range(blocks):
        out_ref[block] = projected[:, block * lane : (block + 1) * lane]


def pack_weights_kernel(gate_ref, up_ref, down_ref, out_ref, held, in_sems, out_sems):
    units = gate_ref.shape[1]
    groups = [
        [pltpu.make_async_copy(gate_ref, held.at[0], in_sems.at[0])],
        [pltpu.make_async_copy(up_ref, held.at[1], in_sems.at[1])],
        [],
    ]
    for block in range(down_ref.shape[1] // units):
        columns = pl.ds(block * units, units)
        groups[2].append(
            pltpu.make_async_copy(
                down_ref.at[:, columns], held.at[2, columns, :], in_sems.at[2 + block]
            )
        )
    for group in groups:
        for copy in group:
            copy.start()
    outward = []
    for kind, group in enumerate(groups):
        for copy in group:
            copy.wait()
        outward.append(pltpu.make_async_copy(held.at[kind], out_ref.at[kind], out_sems.at[kind]))
        outward[kind].start()
    for copy in outward:
        copy.wait()


def expert_kernel(rows_in_ref, gain_ref, *refs):
    sets = len(refs) - 5
    out_ref, rows_ref, hidden_ref, kinds, sems = refs[sets:]
    blocks = rows_in_ref.shape[0]
    width = rows_ref.shape[1]
    units = kinds.shape[3]
    copies = [
        [pltpu.make_async_copy(refs[part].at[kind], kinds.at[part, kind], sems.at[part, kind]) for kind in range(3)]
        for part in range(sets)
    ]
    for part in range(sets):
        copies[part][0].start()
        copies[part][1].start()
    for part in range(sets):
        copies[part][2].start()
    squares = jnp.zeros(rows_in_ref.shape[1:], jnp.float32)
    for block in range(blocks):
        values = rows_in_ref[block].astype(jnp.float32)
        squares = squares + values * values
    scale = lax.rsqrt(jnp.sum(squares, axis=1, keepdims=True) / width + norm_eps)
    for block in range(blocks):
        values = rows_in_ref[block].astype(jnp.float32) * scale * gain_ref[block]
        rows_ref[:, block * lane : (block + 1) * lane] = values.astype(jnp.bfloat16)
    for part in range(sets):
        copies[part][0].wait()
        gate = jnp.dot(rows_ref[...], kinds[part, 0], preferred_element_type=jnp.float32)
        copies[part][1].wait()
        up = jnp.dot(rows_ref[...], kinds[part, 1], preferred_element_type=jnp.float32)
        hidden_ref[part] = (gate / (1.0 + jnp.exp(-gate)) * up).astype(jnp.bfloat16)
    for part in range(sets):
        copies[part][2].wait()
    for block in range(width // units):
        down_rows = slice(block * units, (block + 1) * units)
        total = sum(
            jnp.dot(hidden_ref[part], kinds[part, 2, down_rows, :], preferred_element_type=jnp.float32)
            for part in range(sets)
        ).astype(jnp.bfloat16)
        for piece in range(units // lane):
            out_ref[block * (units // lane) + piece] = total[:, piece * lane : (piece + 1) * lane]


def shards(
    residual,
    queries,
    keys,
    values,
    forget_cache,
    out_weight,
    norm_gain,
    routes,
    route_weight,
    gate_weight,
    up_weight,
    down_weight,
):
    z_count, x_count, y_count = (lax.axis_size(axis) for axis in ("z", "x", "y"))
    sp_count = z_count * x_count
    token_count, local_width = residual.shape
    model_width = norm_gain.shape[0]
    head_count = forget_cache.shape[0]
    head_width = queries.shape[0] // head_count
    top_count = routes.shape[1]
    capacity = max(2, token_count * top_count * 5 // (4 * sp_count))
    slot_total = sp_count * capacity
    bf16, f32 = jnp.bfloat16, jnp.float32
    place = jnp.stack(
        [lax.axis_index("z"), lax.axis_index("x"), lax.axis_index("c"), lax.axis_index("y")]
    ).astype(jnp.int32)
    smem = pl.BlockSpec(memory_space=pltpu.SMEM)
    vmem = pl.BlockSpec(memory_space=pltpu.VMEM)

    deep = head_width + extra_rows
    message_rows = 2 * head_count * head_width + gate_rows
    message, scaled = pl.pallas_call(
        functools.partial(pack_kernel, head_width),
        out_shape=(
            jax.ShapeDtypeStruct((z_count, message_rows, token_count), bf16),
            kept(queries.shape, bf16),
        ),
        in_specs=[vmem] * 4,
        out_specs=(vmem, vmem),
        name="pack",
        interpret=INTERPRET,
    )(keys, values, forget_cache, queries)
    gathered = lax.all_to_all(message, "z", split_axis=0, concat_axis=0, tiled=True)
    query_list = [scaled] + [
        lax.ppermute(scaled, "x", [(i, (i + shift) % x_count) for i in range(x_count)])
        for shift in range(1, x_count)
    ]
    slice_moves = []
    for y_from in range(y_count):
        slice_moves.append((2 * y_from, 2 * ((y_from - 1) % y_count)))
        slice_moves.append((2 * y_from + 1, 2 * ((y_from + 1) % y_count) + 1))
    hidden_units = gate_weight.shape[2]
    any_space = pl.BlockSpec(memory_space=pl.ANY)
    down_blocks = model_width // hidden_units
    own_set = pl.pallas_call(
        pack_weights_kernel,
        out_shape=jax.ShapeDtypeStruct((3, model_width, hidden_units), bf16),
        in_specs=[any_space] * 3,
        out_specs=any_space,
        scratch_shapes=[
            pltpu.VMEM((3, model_width, hidden_units), bf16),
            pltpu.SemaphoreType.DMA((2 + down_blocks,)),
            pltpu.SemaphoreType.DMA((3,)),
        ],
        name="pack_weights",
        interpret=INTERPRET,
    )(gate_weight[0], up_weight[0], down_weight[0])
    near_set = lax.ppermute(own_set, TP, slice_moves)
    own_swapped = swapped(own_set)
    far_out_weight = swapped(out_weight)
    near_swapped = swapped(near_set)
    attend = pl.pallas_call(
        functools.partial(attend_kernel, head_count, head_width),
        out_shape=jax.ShapeDtypeStruct(
            (x_count, 2, head_count * head_width + extra_rows, token_count), bf16
        ),
        in_specs=[smem] + [vmem] * (1 + x_count),
        out_specs=vmem,
        scratch_shapes=[
            pltpu.VMEM((head_count, deep, x_count * token_count), bf16),
            pltpu.VMEM((head_count, deep, z_count * token_count), bf16),
            pltpu.VMEM((head_count, deep, z_count * token_count), bf16),
        ],
        name="attend",
        interpret=INTERPRET,
    )
    parts = attend(place, held(gathered), *map(held, query_list))
    part_shape = parts.shape
    received = lax.all_to_all(
        parts.reshape(2 * x_count, *part_shape[2:]), ("x", "c"), split_axis=0, concat_axis=0, tiled=True
    ).reshape(part_shape)

    expert_ids = jnp.arange(sp_count, dtype=jnp.int32)
    chosen = routes[:, :, None] == expert_ids
    named = jnp.any(chosen, axis=1)
    token_ids = jnp.arange(token_count, dtype=jnp.int32)
    before = (token_ids[None, :] < token_ids[:, None]).astype(bf16)
    rank = jnp.dot(before, named.astype(bf16), preferred_element_type=f32).astype(jnp.int32)
    slot_ids = jnp.arange(capacity, dtype=jnp.int32)
    taken = (named.T[:, None, :] & (rank.T[:, None, :] == slot_ids[:, None])).astype(bf16)
    taken = taken.reshape(slot_total, token_count)
    share = jnp.sum(jnp.where(chosen, route_weight[:, :, None], 0.0), axis=1)
    share_first = lax.reduce_precision(share, 8, 7)
    share_rest = (share - share_first).astype(bf16)

    def spread(weights):
        return jnp.where(
            rank[:, :, None] == slot_ids, weights.astype(bf16)[:, :, None], jnp.zeros((), bf16)
        ).reshape(token_count, slot_total)

    give_first, give_rest = spread(share_first), spread(share_rest)

    projected = pl.pallas_call(
        functools.partial(project_kernel, head_count, head_width),
        out_shape=jax.ShapeDtypeStruct((y_count, token_count, local_width), bf16),
        in_specs=[smem, vmem, vmem, vmem],
        out_specs=vmem,
        scratch_shapes=[pltpu.VMEM((2 * head_count * head_width, y_count * local_width), bf16)],
        name="project",
        interpret=INTERPRET,
    )(place, held(received), held(out_weight), held(far_out_weight))
    pieces = lax.all_to_all(projected, "y", split_axis=0, concat_axis=0, tiled=True)
    pieces, own_swapped, near_set, near_swapped = lax.optimization_barrier(
        (pieces, own_swapped, near_set, near_swapped)
    )
    weight_sets = [own_set, own_swapped, near_set, near_swapped]
    head_sum = jnp.sum(pieces.astype(f32), axis=0)
    stream = (residual.astype(f32) + head_sum).astype(bf16)

    sent = jnp.dot(taken, stream, preferred_element_type=f32).astype(bf16)
    arrived = lax.all_to_all(sent.reshape(sp_count, capacity, local_width), SP, split_axis=0, concat_axis=0, tiled=True)
    quarter = slot_total // 4
    arrived = arrived.reshape(4, quarter, local_width)
    copies = jnp.broadcast_to(arrived, (y_count // 2, *arrived.shape))
    rows = lax.all_to_all(
        copies.reshape(2 * y_count, quarter, local_width), TP, split_axis=0, concat_axis=0, tiled=True
    )
    sets = len(weight_sets)
    out_rows = pl.pallas_call(
        expert_kernel,
        out_shape=kept((2 * y_count, quarter, local_width), bf16),
        in_specs=[vmem, vmem] + [any_space] * sets,
        out_specs=vmem,
        scratch_shapes=[
            pltpu.VMEM((quarter, model_width), bf16),
            pltpu.VMEM((sets, quarter, hidden_units), bf16),
            pltpu.VMEM((sets, 3, model_width, hidden_units), bf16),
            pltpu.SemaphoreType.DMA((sets, 3)),
        ],
        name="expert",
        interpret=INTERPRET,
    )(held(rows), norm_gain.reshape(2 * y_count, 1, lane), *weight_sets)
    pieces = lax.all_to_all(out_rows, TP, split_axis=0, concat_axis=0, tiled=True)
    expert_out = jnp.sum(
        pieces.reshape(y_count // 2, 4, quarter, local_width).astype(f32), axis=0
    ).astype(bf16)
    back = lax.all_to_all(
        expert_out.reshape(sp_count, capacity, local_width), SP, split_axis=0, concat_axis=0, tiled=True
    ).reshape(slot_total, local_width)
    mixture = jnp.dot(give_first, back, preferred_element_type=f32) + jnp.dot(
        give_rest, back, preferred_element_type=f32
    )
    return (stream.astype(f32) + mixture).astype(bf16)


def solution(mesh):
    sp_count, tp_count = mesh.shape["sp"], mesh.shape["tp"]
    x_count = 4 if sp_count % 8 == 0 else 2
    finer = Mesh(
        mesh.devices.reshape(sp_count // x_count, x_count, tp_count // 2, 2), ("z", "x", "y", "c")
    )
    in_specs = (
        P(SP, TP),
        P(TP, SP),
        P(TP, SP),
        P(TP, SP),
        P(TP, SP),
        P(TP, None),
        P(),
        P(SP, None),
        P(SP, None),
        P(SP, None, TP),
        P(SP, None, TP),
        P(SP, TP, None),
    )
    return jax.shard_map(shards, mesh=finer, in_specs=in_specs, out_specs=P(SP, TP), check_vma=False)
```

```python
import functools

import jax
import jax.numpy as jnp
from jax import lax
from jax.experimental import pallas as pl
from jax.experimental.pallas import tpu as pltpu
from jax.sharding import Mesh
from jax.sharding import PartitionSpec as P


SP = ("z", "x")
TP = ("y", "c")
INTERPRET = False

norm_eps = 1e-06
masked_score = -1e30
extra_rows = 16
gate_rows = 8
lane = 128


def held(array):
    return array if INTERPRET else pltpu.with_memory_space_constraint(array, pltpu.VMEM)


def kept(shape, dtype):
    return jax.ShapeDtypeStruct(shape, dtype) if INTERPRET else pltpu.VMEM(shape, dtype)


def swapped(shard):
    return lax.ppermute(shard, "c", [(0, 1), (1, 0)])


def three_parts(full):
    parts = []
    for _ in range(3):
        part = full.astype(jnp.bfloat16).astype(jnp.float32)
        full = full - part
        parts.append(part)
    return parts


def pack_kernel(head_width, keys_ref, values_ref, gates_ref, queries_ref, out_ref, query_ref):
    tokens = keys_ref.shape[1]
    head_count = gates_ref.shape[0]
    row = lax.broadcasted_iota(jnp.int32, (extra_rows, tokens), 0)
    gates = jnp.zeros((extra_rows, tokens), jnp.float32)
    for head in range(head_count):
        for place, part in enumerate(three_parts(gates_ref[head : head + 1])):
            gates = jnp.where(row == 3 * head + place, part, gates)
    message = jnp.concatenate(
        [keys_ref[...], values_ref[...], gates[:gate_rows].astype(jnp.bfloat16)], axis=0
    )
    for copy in range(out_ref.shape[0]):
        out_ref[copy] = message
    query_ref[...] = queries_ref[...] * jnp.asarray(head_width ** (-0.5), jnp.bfloat16)


def attend_kernel(head_count, head_width, place_ref, kv_ref, *refs):
    out_ref, query_scratch, key_scratch, value_scratch = refs[-4:]
    query_refs = refs[:-4]
    tokens = kv_ref.shape[2]
    z_count, x_count = kv_ref.shape[0], len(query_refs)
    z_place, x_place = place_ref[0], place_ref[1]
    row = lax.broadcasted_iota(jnp.int32, (extra_rows, tokens), 0)
    ones = jnp.ones((extra_rows, tokens), jnp.bfloat16)
    for head in range(head_count):
        counted = ((row >= 3 * head) & (row < 3 * head + 3)) | (row == gate_rows - 1)
        minus = jnp.where(counted, -1.0, 0.0).astype(jnp.bfloat16)
        rows = slice(head * head_width, (head + 1) * head_width)
        for shift in range(x_count):
            target = lax.rem(x_place + x_count - shift, x_count)
            columns = pl.ds(pl.multiple_of(target * tokens, tokens), tokens)
            query_scratch[head, :head_width, columns] = query_refs[shift][rows]
            query_scratch[head, head_width:, columns] = minus
        for block in range(z_count):
            source = lax.rem(z_place + block, z_count)
            columns = slice(block * tokens, (block + 1) * tokens)
            first = (head_count + head) * head_width
            later = jnp.where((block > 0) & (z_place + block < z_count), -2 * masked_score, 0.0)
            gates = kv_ref[source, 2 * head_count * head_width :]
            key_scratch[head, :head_width, columns] = kv_ref[source, rows]
            gates = jnp.where(row[:gate_rows] == gate_rows - 1, later, gates.astype(jnp.float32))
            gates = jnp.concatenate([gates, jnp.zeros_like(gates)], axis=0)
            key_scratch[head, head_width:, columns] = gates.astype(jnp.bfloat16)
            value_scratch[head, :head_width, columns] = kv_ref[source, first : first + head_width]
            value_scratch[head, head_width:, columns] = ones
    wide = x_count * tokens
    stats = [jnp.zeros((extra_rows, tokens), jnp.float32)] * x_count
    for head in range(head_count):
        rows = slice(head * head_width, (head + 1) * head_width)
        for first in range(0, x_count * tokens, wide):
            scores = lax.dot_general(
                key_scratch[head],
                query_scratch[head, :, first : first + wide],
                (((0,), (0,)), ((), ())),
                preferred_element_type=jnp.float32,
            )
            near = scores[:tokens]
            key_place = lax.broadcasted_iota(jnp.int32, near.shape, 0) + x_place * tokens
            query_place = lax.broadcasted_iota(jnp.int32, near.shape, 1) + first
            near = jnp.where(key_place <= query_place, near, 2 * masked_score)
            rest = scores[tokens:]
            peak = jnp.maximum(jnp.max(near, axis=0, keepdims=True), jnp.max(rest, axis=0, keepdims=True))
            peak = jnp.maximum(peak, masked_score)
            near_weights = jnp.exp(near - peak).astype(jnp.bfloat16)
            rest_weights = jnp.exp(rest - peak).astype(jnp.bfloat16)
            summed = jnp.dot(
                value_scratch[head, :, :tokens], near_weights, preferred_element_type=jnp.float32
            ) + jnp.dot(value_scratch[head, :, tokens:], rest_weights, preferred_element_type=jnp.float32)
            for block in range(first // tokens, (first + wide) // tokens):
                columns = slice(block * tokens - first, (block + 1) * tokens - first)
                part_sum = summed[:head_width, columns].astype(jnp.bfloat16)
                total = summed[head_width : head_width + 1, columns]
                for place, part in enumerate(three_parts(peak[:, columns]) + three_parts(total)):
                    stats[block] = jnp.where(row == 6 * head + place, part, stats[block])
                for core in range(2):
                    out_ref[block, core, rows] = part_sum
    for block in range(x_count):
        for core in range(2):
            out_ref[block, core, head_count * head_width :] = stats[block].astype(jnp.bfloat16)


def project_kernel(head_count, head_width, place_ref, parts_ref, weight_ref, far_weight_ref, out_ref, weight_scratch):
    x_count = parts_ref.shape[0]
    blocks = out_ref.shape[0]
    width = head_count * head_width
    core = place_ref[2]
    rows = []
    for side, at in ((0, core), (1, 1 - core)):
        source = (weight_ref, far_weight_ref)[side]
        for block in range(blocks):
            columns = pl.ds(pl.multiple_of((block * 2 + core) * lane, lane), lane)
            weight_scratch[side * width : (side + 1) * width, block * lane : (block + 1) * lane] = (
                source[:, columns]
            )
        stats = [parts_ref[part, at, width:].astype(jnp.float32) for part in range(x_count)]
        for head in range(head_count):
            base = 6 * head
            peaks = [
                kept[base : base + 1] + kept[base + 1 : base + 2] + kept[base + 2 : base + 3]
                for kept in stats
            ]
            totals = [
                kept[base + 3 : base + 4] + kept[base + 4 : base + 5] + kept[base + 5 : base + 6]
                for kept in stats
            ]
            top = functools.reduce(jnp.maximum, peaks)
            factors = [jnp.exp(peak - top) for peak in peaks]
            total = sum(factor * amount for factor, amount in zip(factors, totals))
            summed = sum(
                parts_ref[part, at, head * head_width : (head + 1) * head_width].astype(jnp.float32)
                * factors[part]
                for part in range(x_count)
            )
            rows.append((summed / total).astype(jnp.bfloat16))
    attended = jnp.concatenate(rows, axis=0)
    projected = lax.dot_general(
        attended, weight_scratch[...], (((0,), (0,)), ((), ())), preferred_element_type=jnp.float32
    ).astype(jnp.bfloat16)
    for block in range(blocks):
        out_ref[block] = projected[:, block * lane : (block + 1) * lane]


def pack_weights_kernel(gate_ref, up_ref, down_ref, out_ref, held, in_sems, out_sems):
    units = gate_ref.shape[1]
    groups = [
        [pltpu.make_async_copy(gate_ref, held.at[0], in_sems.at[0])],
        [pltpu.make_async_copy(up_ref, held.at[1], in_sems.at[1])],
        [],
    ]
    for block in range(down_ref.shape[1] // units):
        columns = pl.ds(block * units, units)
        groups[2].append(
            pltpu.make_async_copy(
                down_ref.at[:, columns], held.at[2, columns, :], in_sems.at[2 + block]
            )
        )
    for group in groups:
        for copy in group:
            copy.start()
    outward = []
    for kind, group in enumerate(groups):
        for copy in group:
            copy.wait()
        outward.append(pltpu.make_async_copy(held.at[kind], out_ref.at[kind], out_sems.at[kind]))
        outward[kind].start()
    for copy in outward:
        copy.wait()


def expert_kernel(rows_in_ref, gain_ref, *refs):
    sets = len(refs) - 5
    out_ref, rows_ref, hidden_ref, kinds, sems = refs[sets:]
    blocks = rows_in_ref.shape[0]
    width = rows_ref.shape[1]
    units = kinds.shape[3]
    copies = [
        [pltpu.make_async_copy(refs[part].at[kind], kinds.at[part, kind], sems.at[part, kind]) for kind in range(3)]
        for part in range(sets)
    ]
    for part in range(sets):
        copies[part][0].start()
        copies[part][1].start()
    for part in range(sets):
        copies[part][2].start()
    squares = jnp.zeros(rows_in_ref.shape[1:], jnp.float32)
    for block in range(blocks):
        values = rows_in_ref[block].astype(jnp.float32)
        squares = squares + values * values
    scale = lax.rsqrt(jnp.sum(squares, axis=1, keepdims=True) / width + norm_eps)
    for block in range(blocks):
        values = rows_in_ref[block].astype(jnp.float32) * scale * gain_ref[block]
        rows_ref[:, block * lane : (block + 1) * lane] = values.astype(jnp.bfloat16)
    for part in range(sets):
        copies[part][0].wait()
        gate = jnp.dot(rows_ref[...], kinds[part, 0], preferred_element_type=jnp.float32)
        copies[part][1].wait()
        up = jnp.dot(rows_ref[...], kinds[part, 1], preferred_element_type=jnp.float32)
        hidden_ref[part] = (gate / (1.0 + jnp.exp(-gate)) * up).astype(jnp.bfloat16)
    for part in range(sets):
        copies[part][2].wait()
    for block in range(width // units):
        down_rows = slice(block * units, (block + 1) * units)
        total = sum(
            jnp.dot(hidden_ref[part], kinds[part, 2, down_rows, :], preferred_element_type=jnp.float32)
            for part in range(sets)
        ).astype(jnp.bfloat16)
        for piece in range(units // lane):
            out_ref[block * (units // lane) + piece] = total[:, piece * lane : (piece + 1) * lane]


def shards(
    residual,
    queries,
    keys,
    values,
    forget_cache,
    out_weight,
    norm_gain,
    routes,
    route_weight,
    gate_weight,
    up_weight,
    down_weight,
):
    z_count, x_count, y_count = (lax.axis_size(axis) for axis in ("z", "x", "y"))
    sp_count = z_count * x_count
    token_count, local_width = residual.shape
    model_width = norm_gain.shape[0]
    head_count = forget_cache.shape[0]
    head_width = queries.shape[0] // head_count
    top_count = routes.shape[1]
    capacity = max(2, token_count * top_count * 5 // (4 * sp_count))
    slot_total = sp_count * capacity
    bf16, f32 = jnp.bfloat16, jnp.float32
    place = jnp.stack(
        [lax.axis_index("z"), lax.axis_index("x"), lax.axis_index("c"), lax.axis_index("y")]
    ).astype(jnp.int32)
    smem = pl.BlockSpec(memory_space=pltpu.SMEM)
    vmem = pl.BlockSpec(memory_space=pltpu.VMEM)

    deep = head_width + extra_rows
    message_rows = 2 * head_count * head_width + gate_rows
    message, scaled = pl.pallas_call(
        functools.partial(pack_kernel, head_width),
        out_shape=(
            jax.ShapeDtypeStruct((z_count, message_rows, token_count), bf16),
            kept(queries.shape, bf16),
        ),
        in_specs=[vmem] * 4,
        out_specs=(vmem, vmem),
        name="pack",
        interpret=INTERPRET,
    )(keys, values, forget_cache, queries)
    gathered = lax.all_to_all(message, "z", split_axis=0, concat_axis=0, tiled=True)
    query_list = [scaled] + [
        lax.ppermute(scaled, "x", [(i, (i + shift) % x_count) for i in range(x_count)])
        for shift in range(1, x_count)
    ]
    slice_moves = []
    for y_from in range(y_count):
        slice_moves.append((2 * y_from, 2 * ((y_from - 1) % y_count)))
        slice_moves.append((2 * y_from + 1, 2 * ((y_from + 1) % y_count) + 1))
    hidden_units = gate_weight.shape[2]
    any_space = pl.BlockSpec(memory_space=pl.ANY)
    down_blocks = model_width // hidden_units
    own_set = pl.pallas_call(
        pack_weights_kernel,
        out_shape=jax.ShapeDtypeStruct((3, model_width, hidden_units), bf16),
        in_specs=[any_space] * 3,
        out_specs=any_space,
        scratch_shapes=[
            pltpu.VMEM((3, model_width, hidden_units), bf16),
            pltpu.SemaphoreType.DMA((2 + down_blocks,)),
            pltpu.SemaphoreType.DMA((3,)),
        ],
        name="pack_weights",
        interpret=INTERPRET,
    )(gate_weight[0], up_weight[0], down_weight[0])
    near_set = lax.ppermute(own_set, TP, slice_moves)
    own_swapped = swapped(own_set)
    far_out_weight = swapped(out_weight)
    near_swapped = swapped(near_set)
    expert_ids = jnp.arange(sp_count, dtype=jnp.int32)
    chosen = routes[:, :, None] == expert_ids
    named = jnp.any(chosen, axis=1)
    token_ids = jnp.arange(token_count, dtype=jnp.int32)
    before = (token_ids[None, :] < token_ids[:, None]).astype(bf16)
    rank = jnp.dot(before, named.astype(bf16), preferred_element_type=f32).astype(jnp.int32)
    slot_ids = jnp.arange(capacity, dtype=jnp.int32)
    taken = (named.T[:, None, :] & (rank.T[:, None, :] == slot_ids[:, None])).astype(bf16)
    taken = taken.reshape(slot_total, token_count)
    share = jnp.sum(jnp.where(chosen, route_weight[:, :, None], 0.0), axis=1)
    share_first = lax.reduce_precision(share, 8, 7)
    share_rest = (share - share_first).astype(bf16)

    gathered, taken = lax.optimization_barrier((gathered, taken))
    attend = pl.pallas_call(
        functools.partial(attend_kernel, head_count, head_width),
        out_shape=jax.ShapeDtypeStruct(
            (x_count, 2, head_count * head_width + extra_rows, token_count), bf16
        ),
        in_specs=[smem] + [vmem] * (1 + x_count),
        out_specs=vmem,
        scratch_shapes=[
            pltpu.VMEM((head_count, deep, x_count * token_count), bf16),
            pltpu.VMEM((head_count, deep, z_count * token_count), bf16),
            pltpu.VMEM((head_count, deep, z_count * token_count), bf16),
        ],
        name="attend",
        interpret=INTERPRET,
    )
    parts = attend(place, held(gathered), *map(held, query_list))
    part_shape = parts.shape
    received = lax.all_to_all(
        parts.reshape(2 * x_count, *part_shape[2:]), ("x", "c"), split_axis=0, concat_axis=0, tiled=True
    ).reshape(part_shape)
    received, own_swapped = lax.optimization_barrier((received, own_swapped))

    def spread(weights):
        return jnp.where(
            rank[:, :, None] == slot_ids, weights.astype(bf16)[:, :, None], jnp.zeros((), bf16)
        ).reshape(token_count, slot_total)

    give_first, give_rest = spread(share_first), spread(share_rest)

    projected = pl.pallas_call(
        functools.partial(project_kernel, head_count, head_width),
        out_shape=kept((y_count, token_count, local_width), bf16),
        in_specs=[smem, vmem, vmem, vmem],
        out_specs=vmem,
        scratch_shapes=[pltpu.VMEM((2 * head_count * head_width, y_count * local_width), bf16)],
        name="project",
        interpret=INTERPRET,
    )(place, held(received), held(out_weight), held(far_out_weight))
    pieces = lax.all_to_all(projected, "y", split_axis=0, concat_axis=0, tiled=True)
    weight_sets = [own_set, own_swapped, near_set, near_swapped]
    head_sum = jnp.sum(pieces.astype(f32), axis=0)
    stream = (residual.astype(f32) + head_sum).astype(bf16)

    sent = jnp.dot(taken, stream, preferred_element_type=f32).astype(bf16)
    arrived = lax.all_to_all(sent.reshape(sp_count, capacity, local_width), SP, split_axis=0, concat_axis=0, tiled=True)
    quarter = slot_total // 4
    arrived = arrived.reshape(4, quarter, local_width)
    copies = jnp.broadcast_to(arrived, (y_count // 2, *arrived.shape))
    rows = lax.all_to_all(
        copies.reshape(2 * y_count, quarter, local_width), TP, split_axis=0, concat_axis=0, tiled=True
    )
    sets = len(weight_sets)
    out_rows = pl.pallas_call(
        expert_kernel,
        out_shape=kept((2 * y_count, quarter, local_width), bf16),
        in_specs=[vmem, vmem] + [any_space] * sets,
        out_specs=vmem,
        scratch_shapes=[
            pltpu.VMEM((quarter, model_width), bf16),
            pltpu.VMEM((sets, quarter, hidden_units), bf16),
            pltpu.VMEM((sets, 3, model_width, hidden_units), bf16),
            pltpu.SemaphoreType.DMA((sets, 3)),
        ],
        name="expert",
        interpret=INTERPRET,
    )(held(rows), norm_gain.reshape(2 * y_count, 1, lane), *weight_sets)
    pieces = lax.all_to_all(out_rows, TP, split_axis=0, concat_axis=0, tiled=True)
    expert_out = jnp.sum(
        pieces.reshape(y_count // 2, 4, quarter, local_width).astype(f32), axis=0
    ).astype(bf16)
    back = lax.all_to_all(
        expert_out.reshape(sp_count, capacity, local_width), SP, split_axis=0, concat_axis=0, tiled=True
    ).reshape(slot_total, local_width)
    mixture = jnp.dot(give_first, back, preferred_element_type=f32) + jnp.dot(
        give_rest, back, preferred_element_type=f32
    )
    return (stream.astype(f32) + mixture).astype(bf16)


def solution(mesh):
    sp_count, tp_count = mesh.shape["sp"], mesh.shape["tp"]
    x_count = 4 if sp_count % 8 == 0 else 2
    finer = Mesh(
        mesh.devices.reshape(sp_count // x_count, x_count, tp_count // 2, 2), ("z", "x", "y", "c")
    )
    in_specs = (
        P(SP, TP),
        P(TP, SP),
        P(TP, SP),
        P(TP, SP),
        P(TP, SP),
        P(TP, None),
        P(),
        P(SP, None),
        P(SP, None),
        P(SP, None, TP),
        P(SP, None, TP),
        P(SP, TP, None),
    )
    return jax.shard_map(shards, mesh=finer, in_specs=in_specs, out_specs=P(SP, TP), check_vma=False)
```

```python
import functools

import jax
import jax.numpy as jnp
from jax import lax
from jax.experimental import pallas as pl
from jax.experimental.pallas import tpu as pltpu
from jax.sharding import Mesh
from jax.sharding import PartitionSpec as P


SP = ("z", "x")
TP = ("y", "c")
INTERPRET = False

norm_eps = 1e-06
masked_score = -1e30
extra_rows = 16
gate_rows = 8
lane = 128


def held(array):
    return array if INTERPRET else pltpu.with_memory_space_constraint(array, pltpu.VMEM)


def kept(shape, dtype):
    return jax.ShapeDtypeStruct(shape, dtype) if INTERPRET else pltpu.VMEM(shape, dtype)


def swapped(shard):
    return lax.ppermute(shard, "c", [(0, 1), (1, 0)])


def three_parts(full):
    parts = []
    for _ in range(3):
        part = full.astype(jnp.bfloat16).astype(jnp.float32)
        full = full - part
        parts.append(part)
    return parts


def pack_kernel(head_width, keys_ref, values_ref, gates_ref, queries_ref, out_ref, query_ref):
    tokens = keys_ref.shape[1]
    head_count = gates_ref.shape[0]
    row = lax.broadcasted_iota(jnp.int32, (extra_rows, tokens), 0)
    gates = jnp.zeros((extra_rows, tokens), jnp.float32)
    for head in range(head_count):
        for place, part in enumerate(three_parts(gates_ref[head : head + 1])):
            gates = jnp.where(row == 3 * head + place, part, gates)
    message = jnp.concatenate(
        [keys_ref[...], values_ref[...], gates[:gate_rows].astype(jnp.bfloat16)], axis=0
    )
    for copy in range(out_ref.shape[0]):
        out_ref[copy] = message
    query_ref[...] = queries_ref[...] * jnp.asarray(head_width ** (-0.5), jnp.bfloat16)


def attend_kernel(head_count, head_width, place_ref, kv_ref, *refs):
    out_ref, query_scratch, key_scratch, value_scratch = refs[-4:]
    query_refs = refs[:-4]
    tokens = kv_ref.shape[2]
    z_count, x_count = kv_ref.shape[0], len(query_refs)
    z_place, x_place = place_ref[0], place_ref[1]
    row = lax.broadcasted_iota(jnp.int32, (extra_rows, tokens), 0)
    ones = jnp.ones((extra_rows, tokens), jnp.bfloat16)
    for head in range(head_count):
        counted = ((row >= 3 * head) & (row < 3 * head + 3)) | (row == gate_rows - 1)
        minus = jnp.where(counted, -1.0, 0.0).astype(jnp.bfloat16)
        rows = slice(head * head_width, (head + 1) * head_width)
        for shift in range(x_count):
            target = lax.rem(x_place + x_count - shift, x_count)
            columns = pl.ds(pl.multiple_of(target * tokens, tokens), tokens)
            query_scratch[head, :head_width, columns] = query_refs[shift][rows]
            query_scratch[head, head_width:, columns] = minus
        for block in range(z_count):
            source = lax.rem(z_place + block, z_count)
            columns = slice(block * tokens, (block + 1) * tokens)
            first = (head_count + head) * head_width
            later = jnp.where((block > 0) & (z_place + block < z_count), -2 * masked_score, 0.0)
            gates = kv_ref[source, 2 * head_count * head_width :]
            key_scratch[head, :head_width, columns] = kv_ref[source, rows]
            gates = jnp.where(row[:gate_rows] == gate_rows - 1, later, gates.astype(jnp.float32))
            gates = jnp.concatenate([gates, jnp.zeros_like(gates)], axis=0)
            key_scratch[head, head_width:, columns] = gates.astype(jnp.bfloat16)
            value_scratch[head, :head_width, columns] = kv_ref[source, first : first + head_width]
            value_scratch[head, head_width:, columns] = ones
    wide = x_count * tokens
    stats = [jnp.zeros((extra_rows, tokens), jnp.float32)] * x_count
    for head in range(head_count):
        rows = slice(head * head_width, (head + 1) * head_width)
        for first in range(0, x_count * tokens, wide):
            scores = lax.dot_general(
                key_scratch[head],
                query_scratch[head, :, first : first + wide],
                (((0,), (0,)), ((), ())),
                preferred_element_type=jnp.float32,
            )
            near = scores[:tokens]
            key_place = lax.broadcasted_iota(jnp.int32, near.shape, 0) + x_place * tokens
            query_place = lax.broadcasted_iota(jnp.int32, near.shape, 1) + first
            near = jnp.where(key_place <= query_place, near, 2 * masked_score)
            rest = scores[tokens:]
            peak = jnp.maximum(jnp.max(near, axis=0, keepdims=True), jnp.max(rest, axis=0, keepdims=True))
            peak = jnp.maximum(peak, masked_score)
            near_weights = jnp.exp(near - peak).astype(jnp.bfloat16)
            rest_weights = jnp.exp(rest - peak).astype(jnp.bfloat16)
            summed = jnp.dot(
                value_scratch[head, :, :tokens], near_weights, preferred_element_type=jnp.float32
            ) + jnp.dot(value_scratch[head, :, tokens:], rest_weights, preferred_element_type=jnp.float32)
            for block in range(first // tokens, (first + wide) // tokens):
                columns = slice(block * tokens - first, (block + 1) * tokens - first)
                part_sum = summed[:head_width, columns].astype(jnp.bfloat16)
                total = summed[head_width : head_width + 1, columns]
                for place, part in enumerate(three_parts(peak[:, columns]) + three_parts(total)):
                    stats[block] = jnp.where(row == 6 * head + place, part, stats[block])
                for core in range(2):
                    out_ref[block, core, rows] = part_sum
    for block in range(x_count):
        for core in range(2):
            out_ref[block, core, head_count * head_width :] = stats[block].astype(jnp.bfloat16)


def project_kernel(head_count, head_width, place_ref, parts_ref, weight_ref, far_weight_ref, out_ref, weight_scratch):
    x_count = parts_ref.shape[0]
    blocks = out_ref.shape[0]
    width = head_count * head_width
    core = place_ref[2]
    rows = []
    for side, at in ((0, core), (1, 1 - core)):
        source = (weight_ref, far_weight_ref)[side]
        for block in range(blocks):
            columns = pl.ds(pl.multiple_of((block * 2 + core) * lane, lane), lane)
            weight_scratch[side * width : (side + 1) * width, block * lane : (block + 1) * lane] = (
                source[:, columns]
            )
        stats = [parts_ref[part, at, width:].astype(jnp.float32) for part in range(x_count)]
        for head in range(head_count):
            base = 6 * head
            peaks = [
                kept[base : base + 1] + kept[base + 1 : base + 2] + kept[base + 2 : base + 3]
                for kept in stats
            ]
            totals = [
                kept[base + 3 : base + 4] + kept[base + 4 : base + 5] + kept[base + 5 : base + 6]
                for kept in stats
            ]
            top = functools.reduce(jnp.maximum, peaks)
            factors = [jnp.exp(peak - top) for peak in peaks]
            total = sum(factor * amount for factor, amount in zip(factors, totals))
            summed = sum(
                parts_ref[part, at, head * head_width : (head + 1) * head_width].astype(jnp.float32)
                * factors[part]
                for part in range(x_count)
            )
            rows.append((summed / total).astype(jnp.bfloat16))
    attended = jnp.concatenate(rows, axis=0)
    projected = lax.dot_general(
        attended, weight_scratch[...], (((0,), (0,)), ((), ())), preferred_element_type=jnp.float32
    ).astype(jnp.bfloat16)
    for block in range(blocks):
        out_ref[block] = projected[:, block * lane : (block + 1) * lane]


def pack_weights_kernel(gate_ref, up_ref, down_ref, out_ref, held, in_sems, out_sems):
    units = gate_ref.shape[1]
    groups = [
        [pltpu.make_async_copy(gate_ref, held.at[0], in_sems.at[0])],
        [pltpu.make_async_copy(up_ref, held.at[1], in_sems.at[1])],
        [],
    ]
    for block in range(down_ref.shape[1] // units):
        columns = pl.ds(block * units, units)
        groups[2].append(
            pltpu.make_async_copy(
                down_ref.at[:, columns], held.at[2, columns, :], in_sems.at[2 + block]
            )
        )
    for group in groups:
        for copy in group:
            copy.start()
    outward = []
    for kind, group in enumerate(groups):
        for copy in group:
            copy.wait()
        outward.append(pltpu.make_async_copy(held.at[kind], out_ref.at[kind], out_sems.at[kind]))
        outward[kind].start()
    for copy in outward:
        copy.wait()


def expert_kernel(rows_in_ref, gain_ref, *refs):
    sets = len(refs) - 5
    out_ref, rows_ref, hidden_ref, kinds, sems = refs[sets:]
    blocks = rows_in_ref.shape[0]
    width = rows_ref.shape[1]
    units = kinds.shape[3]
    copies = [
        [pltpu.make_async_copy(refs[part].at[kind], kinds.at[part, kind], sems.at[part, kind]) for kind in range(3)]
        for part in range(sets)
    ]
    for part in range(sets):
        copies[part][0].start()
        copies[part][1].start()
    for part in range(sets):
        copies[part][2].start()
    squares = jnp.zeros(rows_in_ref.shape[1:], jnp.float32)
    for block in range(blocks):
        values = rows_in_ref[block].astype(jnp.float32)
        squares = squares + values * values
    scale = lax.rsqrt(jnp.sum(squares, axis=1, keepdims=True) / width + norm_eps)
    for block in range(blocks):
        place = block % (blocks // 2) * 2 + block // (blocks // 2)
        values = rows_in_ref[block].astype(jnp.float32) * scale * gain_ref[place]
        rows_ref[:, place * lane : (place + 1) * lane] = values.astype(jnp.bfloat16)
    for part in range(sets):
        copies[part][0].wait()
        gate = jnp.dot(rows_ref[...], kinds[part, 0], preferred_element_type=jnp.float32)
        copies[part][1].wait()
        up = jnp.dot(rows_ref[...], kinds[part, 1], preferred_element_type=jnp.float32)
        hidden_ref[part] = (gate / (1.0 + jnp.exp(-gate)) * up).astype(jnp.bfloat16)
    for part in range(sets):
        copies[part][2].wait()
    for block in range(width // units):
        down_rows = slice(block * units, (block + 1) * units)
        total = sum(
            jnp.dot(hidden_ref[part], kinds[part, 2, down_rows, :], preferred_element_type=jnp.float32)
            for part in range(sets)
        ).astype(jnp.bfloat16)
        for piece in range(units // lane):
            place = block * (units // lane) + piece
            out_ref[place % 2 * (blocks // 2) + place // 2] = total[:, piece * lane : (piece + 1) * lane]


def shards(
    residual,
    queries,
    keys,
    values,
    forget_cache,
    out_weight,
    norm_gain,
    routes,
    route_weight,
    gate_weight,
    up_weight,
    down_weight,
):
    z_count, x_count, y_count = (lax.axis_size(axis) for axis in ("z", "x", "y"))
    sp_count = z_count * x_count
    token_count, local_width = residual.shape
    model_width = norm_gain.shape[0]
    head_count = forget_cache.shape[0]
    head_width = queries.shape[0] // head_count
    top_count = routes.shape[1]
    capacity = max(2, token_count * top_count * 5 // (4 * sp_count))
    slot_total = sp_count * capacity
    bf16, f32 = jnp.bfloat16, jnp.float32
    place = jnp.stack(
        [lax.axis_index("z"), lax.axis_index("x"), lax.axis_index("c"), lax.axis_index("y")]
    ).astype(jnp.int32)
    smem = pl.BlockSpec(memory_space=pltpu.SMEM)
    vmem = pl.BlockSpec(memory_space=pltpu.VMEM)

    deep = head_width + extra_rows
    message_rows = 2 * head_count * head_width + gate_rows
    message, scaled = pl.pallas_call(
        functools.partial(pack_kernel, head_width),
        out_shape=(
            jax.ShapeDtypeStruct((z_count, message_rows, token_count), bf16),
            kept(queries.shape, bf16),
        ),
        in_specs=[vmem] * 4,
        out_specs=(vmem, vmem),
        name="pack",
        interpret=INTERPRET,
    )(keys, values, forget_cache, queries)
    gathered = lax.all_to_all(message, "z", split_axis=0, concat_axis=0, tiled=True)
    query_list = [scaled] + [
        lax.ppermute(scaled, "x", [(i, (i + shift) % x_count) for i in range(x_count)])
        for shift in range(1, x_count)
    ]
    slice_moves = []
    for y_from in range(y_count):
        slice_moves.append((2 * y_from, 2 * ((y_from - 1) % y_count)))
        slice_moves.append((2 * y_from + 1, 2 * ((y_from + 1) % y_count) + 1))
    hidden_units = gate_weight.shape[2]
    any_space = pl.BlockSpec(memory_space=pl.ANY)
    down_blocks = model_width // hidden_units
    own_set = pl.pallas_call(
        pack_weights_kernel,
        out_shape=jax.ShapeDtypeStruct((3, model_width, hidden_units), bf16),
        in_specs=[any_space] * 3,
        out_specs=any_space,
        scratch_shapes=[
            pltpu.VMEM((3, model_width, hidden_units), bf16),
            pltpu.SemaphoreType.DMA((2 + down_blocks,)),
            pltpu.SemaphoreType.DMA((3,)),
        ],
        name="pack_weights",
        interpret=INTERPRET,
    )(gate_weight[0], up_weight[0], down_weight[0])
    near_set = lax.ppermute(own_set, TP, slice_moves)
    own_swapped = swapped(own_set)
    far_out_weight = swapped(out_weight)
    near_swapped = swapped(near_set)
    attend = pl.pallas_call(
        functools.partial(attend_kernel, head_count, head_width),
        out_shape=jax.ShapeDtypeStruct(
            (x_count, 2, head_count * head_width + extra_rows, token_count), bf16
        ),
        in_specs=[smem] + [vmem] * (1 + x_count),
        out_specs=vmem,
        scratch_shapes=[
            pltpu.VMEM((head_count, deep, x_count * token_count), bf16),
            pltpu.VMEM((head_count, deep, z_count * token_count), bf16),
            pltpu.VMEM((head_count, deep, z_count * token_count), bf16),
        ],
        name="attend",
        interpret=INTERPRET,
    )
    parts = attend(place, held(gathered), *map(held, query_list))
    part_shape = parts.shape
    received = lax.all_to_all(
        parts.reshape(2 * x_count, *part_shape[2:]), ("x", "c"), split_axis=0, concat_axis=0, tiled=True
    ).reshape(part_shape)

    expert_ids = jnp.arange(sp_count, dtype=jnp.int32)
    chosen = routes[:, :, None] == expert_ids
    named = jnp.any(chosen, axis=1)
    token_ids = jnp.arange(token_count, dtype=jnp.int32)
    before = (token_ids[None, :] < token_ids[:, None]).astype(bf16)
    rank = jnp.dot(before, named.astype(bf16), preferred_element_type=f32).astype(jnp.int32)
    slot_ids = jnp.arange(capacity, dtype=jnp.int32)
    taken = (named.T[:, None, :] & (rank.T[:, None, :] == slot_ids[:, None])).astype(bf16)
    taken = taken.reshape(slot_total, token_count)
    share = jnp.sum(jnp.where(chosen, route_weight[:, :, None], 0.0), axis=1)
    share_first = lax.reduce_precision(share, 8, 7)
    share_rest = (share - share_first).astype(bf16)

    def spread(weights):
        return jnp.where(
            rank[:, :, None] == slot_ids, weights.astype(bf16)[:, :, None], jnp.zeros((), bf16)
        ).reshape(token_count, slot_total)

    give_first, give_rest = spread(share_first), spread(share_rest)

    projected = pl.pallas_call(
        functools.partial(project_kernel, head_count, head_width),
        out_shape=jax.ShapeDtypeStruct((y_count, token_count, local_width), bf16),
        in_specs=[smem, vmem, vmem, vmem],
        out_specs=vmem,
        scratch_shapes=[pltpu.VMEM((2 * head_count * head_width, y_count * local_width), bf16)],
        name="project",
        interpret=INTERPRET,
    )(place, held(received), held(out_weight), held(far_out_weight))
    pieces = lax.all_to_all(projected, "y", split_axis=0, concat_axis=0, tiled=True)
    pieces, own_swapped, near_set, near_swapped = lax.optimization_barrier(
        (pieces, own_swapped, near_set, near_swapped)
    )
    weight_sets = [own_set, own_swapped, near_set, near_swapped]
    head_sum = jnp.sum(pieces.astype(f32), axis=0)
    stream = (residual.astype(f32) + head_sum).astype(bf16)

    sent = jnp.dot(taken, stream, preferred_element_type=f32).astype(bf16)
    arrived = lax.all_to_all(sent.reshape(sp_count, capacity, local_width), SP, split_axis=0, concat_axis=0, tiled=True)
    quarter = slot_total // 4
    arrived = arrived.reshape(4, quarter, local_width)
    by_core = arrived.reshape(2, 2, quarter, local_width).swapaxes(0, 1)
    copies = jnp.broadcast_to(by_core[:, None], (2, y_count // 2, 2, quarter, local_width))
    rows = lax.all_to_all(
        copies.reshape(2 * y_count, quarter, local_width),
        ("c", "y"),
        split_axis=0,
        concat_axis=0,
        tiled=True,
    )
    sets = len(weight_sets)
    out_rows = pl.pallas_call(
        expert_kernel,
        out_shape=kept((2 * y_count, quarter, local_width), bf16),
        in_specs=[vmem, vmem] + [any_space] * sets,
        out_specs=vmem,
        scratch_shapes=[
            pltpu.VMEM((quarter, model_width), bf16),
            pltpu.VMEM((sets, quarter, hidden_units), bf16),
            pltpu.VMEM((sets, 3, model_width, hidden_units), bf16),
            pltpu.SemaphoreType.DMA((sets, 3)),
        ],
        name="expert",
        interpret=INTERPRET,
    )(held(rows), norm_gain.reshape(2 * y_count, 1, lane), *weight_sets)
    pieces = lax.all_to_all(out_rows, ("c", "y"), split_axis=0, concat_axis=0, tiled=True)
    expert_out = jnp.sum(
        pieces.reshape(2, y_count // 2, 2, quarter, local_width).astype(f32), axis=1
    ).astype(bf16).swapaxes(0, 1)
    back = lax.all_to_all(
        expert_out.reshape(sp_count, capacity, local_width), SP, split_axis=0, concat_axis=0, tiled=True
    ).reshape(slot_total, local_width)
    mixture = jnp.dot(give_first, back, preferred_element_type=f32) + jnp.dot(
        give_rest, back, preferred_element_type=f32
    )
    return (stream.astype(f32) + mixture).astype(bf16)


def solution(mesh):
    sp_count, tp_count = mesh.shape["sp"], mesh.shape["tp"]
    x_count = 4 if sp_count % 8 == 0 else 2
    finer = Mesh(
        mesh.devices.reshape(sp_count // x_count, x_count, tp_count // 2, 2), ("z", "x", "y", "c")
    )
    in_specs = (
        P(SP, TP),
        P(TP, SP),
        P(TP, SP),
        P(TP, SP),
        P(TP, SP),
        P(TP, None),
        P(),
        P(SP, None),
        P(SP, None),
        P(SP, None, TP),
        P(SP, None, TP),
        P(SP, TP, None),
    )
    return jax.shard_map(shards, mesh=finer, in_specs=in_specs, out_specs=P(SP, TP), check_vma=False)
```
